512 devices in a mesh: sp: 256 (over z, y, x), tp: 2 (over core).
Axes of the slice: x: 4, y: 8, z: 8, core: 2. Of those that a mesh axis runs over, the one named last changes fastest.
Arguments:
- queries: bfloat16 [131072, 8, 128], P('sp', 'tp'), may hold values from -60 to 60
- keys: bfloat16 [131072, 8, 128], P('sp', 'tp'), may hold values from -40 to 40
- values: bfloat16 [131072, 8, 128], P('sp', 'tp'), may hold values from -6 to 6
- w_out: bfloat16 [1024, 2048], P(None, 'tp'), may hold values from -0.1875 to 0.1875
Outputs:
- mixed: bfloat16 [131072, 2048], P('sp', 'tp')
The draws below stay inside these ranges and needn't reach their ends.
All inputs are finite; a program needn't handle non-finite values.
Results may differ from the reference program's by a relative error of at most 0.0051.
Values may be sent and summed in bfloat16 or wider, within the bound.
No kernel may reach another device: no remote copies, remote signals or barrier semaphores. Data moves between devices by JAX's collectives and lax.ppermute only.
A program may use at most 64 MiB of HBM per device.

```python
import math
import jax
import jax.numpy as jnp
from jax import lax

D = 2048
HEADS = 8
HEAD_DIM = 128
W1 = 128
WINDOW_TWO = 512
DILATION_TWO = 4
WINDOW_THREE = 2048
DILATION_THREE = 16
TOKENS = 131072


def drawn_pair(key):
    shape = (TOKENS, HEADS, HEAD_DIM)
    starting_keys = jax.random.normal(jax.random.fold_in(key, 11), shape, jnp.float32)
    base_queries = jax.random.normal(jax.random.fold_in(key, 12), shape, jnp.float32) * 2.5
    return (jnp.clip(base_queries, -60.0, 60.0), jnp.clip(starting_keys, -40.0, 40.0))


def draw_queries(key, part):
    return drawn_pair(key)[0].astype(jnp.bfloat16)


def draw_keys(key, part):
    return drawn_pair(key)[1].astype(jnp.bfloat16)


def shard_levels(stream_key, dims, split, low, largest):
    def one(position, parts):
        draws = jax.random.uniform(jax.random.fold_in(jax.random.fold_in(stream_key, 6), position), (parts,), jnp.float32, low / len(split), largest / len(split))
        return jnp.repeat(jnp.exp(draws), dims[position] // parts).reshape((-1,) + (1,) * (len(dims) - position - 1))

    gain = one(*split[0])
    for cut in split[1:]:
        gain = gain * one(*cut)
    return gain


def gaussian(stream_key, extent, deviation, bound, shards=(), kind=jnp.bfloat16):
    values = deviation * jax.random.normal(stream_key, extent, jnp.float32)
    if shards:
        values = values * shard_levels(stream_key, extent, shards, -0.22, 0.18)
    return jnp.clip(values, -bound, bound).astype(kind)


def setup_inputs(seed: int = 0) -> dict:
    key_of = jax.random.split(jax.random.key(seed), 5)
    queries = draw_queries(jax.random.fold_in(key_of[4], 71), 0)
    keys = draw_keys(jax.random.fold_in(key_of[4], 71), 0)
    values = gaussian(key_of[2], (TOKENS, HEADS, HEAD_DIM), 1.0, 6.0, ((0, 256), (1, 2)))
    w_out = gaussian(key_of[3], (HEADS * HEAD_DIM, D), (HEADS * HEAD_DIM) ** -0.5, 0.1875, ((1, 2),))
    return dict(queries=queries, keys=keys, values=values, w_out=w_out)


def with_previous(blocks):
    earlier = jnp.concatenate([jnp.zeros_like(blocks[:1]), blocks[:-1]], axis=0)
    return jnp.concatenate([earlier, blocks], axis=1)

def single_branch(head_queries, head_keys, head_values, window, dilation):
    band_rows = window // dilation
    block_count = TOKENS // window
    shape = (block_count, band_rows, dilation, HEAD_DIM)
    query_blocks = head_queries.astype(jnp.float32).reshape(shape)
    key_bands = with_previous(head_keys.astype(jnp.float32).reshape(shape))
    value_bands = with_previous(head_values.astype(jnp.float32).reshape(shape))
    scores = jnp.einsum('nqrd,nkrd->nrqk', query_blocks, key_bands) / math.sqrt(HEAD_DIM)
    query_idx = jnp.arange(band_rows, dtype=jnp.int32)[:, None]
    key_idx = jnp.arange(2 * band_rows, dtype=jnp.int32)[None, :]
    distance = query_idx - key_idx + band_rows
    key_rows = jnp.arange(block_count, dtype=jnp.int32)[:, None, None] * band_rows - band_rows + key_idx[None]
    allowed = (distance >= 0)[None] & (distance <= band_rows)[None] & (key_rows >= 0)
    scores = jnp.where(allowed[:, None], scores, -jnp.inf)
    row_max = lax.optimization_barrier(jnp.max(scores, axis=-1, keepdims=True))
    numerators = jnp.exp(scores - row_max)
    row_sum = lax.optimization_barrier(jnp.sum(numerators, axis=-1, keepdims=True))
    rounded = lax.optimization_barrier(numerators.astype(jnp.bfloat16)).astype(jnp.float32)
    branch_out = jnp.einsum('nrqk,nkrd->nqrd', rounded, value_bands) / jnp.transpose(row_sum, (0, 2, 1, 3))
    log_total = jnp.transpose((row_max + jnp.log(row_sum))[..., 0], (0, 2, 1))
    return (branch_out.reshape(TOKENS, HEAD_DIM), log_total.reshape(TOKENS))

def one_head(operands):
    head_queries, head_keys, head_values = operands
    first_out, first_total = single_branch(head_queries, head_keys, head_values, W1, 1)
    second_output, second_branch_total = single_branch(head_queries, head_keys, head_values, WINDOW_TWO, DILATION_TWO)
    third_output, third_branch_total = single_branch(head_queries, head_keys, head_values, WINDOW_THREE, DILATION_THREE)
    weights = jax.nn.softmax(jnp.stack([first_total, second_branch_total, third_branch_total]), axis=0)
    stacked = jnp.stack([first_out, second_output, third_output])
    return lax.optimization_barrier(jnp.sum(weights[:, :, None] * stacked, axis=0))

def reference(queries, keys, values, w_out):
    per_head = lax.map(one_head, (jnp.transpose(queries, (1, 0, 2)), jnp.transpose(keys, (1, 0, 2)), jnp.transpose(values, (1, 0, 2))))
    attended = jnp.transpose(per_head, (1, 0, 2)).reshape(TOKENS, HEADS * HEAD_DIM).astype(jnp.bfloat16)
    return jnp.dot(attended, w_out, preferred_element_type=jnp.float32).astype(jnp.bfloat16)
```

```python
import math

import jax
import jax.numpy as jnp
from jax import lax
from jax.experimental import pallas as pl
from jax.experimental.pallas import tpu as pltpu
from jax.sharding import Mesh
from jax.sharding import PartitionSpec as P

DILATION_TWO = 4
DILATION_THREE = 16
HEAD_DIM = 128
ROW_CHIPS = 4
BLOCK = 512
STEPS = BLOCK // DILATION_THREE
TILE = 128
SCALE = math.log2(math.e) / math.sqrt(HEAD_DIM)
LOWEST = -1e30
VMEM = pl.BlockSpec(memory_space=pltpu.VMEM)
SMEM = pl.BlockSpec(memory_space=pltpu.SMEM)


def pack_kernel(*refs):
    count = len(refs) // 2
    wide = refs[-1]
    for in_ref, out_ref in zip(refs[:count], refs[count : 2 * count]):
        wide[...] = in_ref[...].astype(jnp.float32)
        for head in range(4):
            for res in range(DILATION_THREE):
                rows = wide[pl.ds(4 * res + head, STEPS, stride=4 * DILATION_THREE), :]
                out_ref[head, res * STEPS : (res + 1) * STEPS, :] = rows.astype(jnp.bfloat16)


def pack(*arrays):
    shape = jax.ShapeDtypeStruct((4, BLOCK, HEAD_DIM), jnp.bfloat16)
    return pl.pallas_call(
        pack_kernel,
        out_shape=[shape] * len(arrays),
        in_specs=[VMEM] * len(arrays),
        out_specs=[VMEM] * len(arrays),
        scratch_shapes=[pltpu.VMEM((4 * BLOCK, HEAD_DIM), jnp.float32)],
        cost_estimate=pl.CostEstimate(
            flops=1000000, bytes_accessed=2 * 524288 * len(arrays), transcendentals=0
        ),
    )(*[array.reshape(4 * BLOCK, HEAD_DIM) for array in arrays])


def masks(order):
    q = lax.broadcasted_iota(jnp.int32, (TILE, TILE), 0)
    k = lax.broadcasted_iota(jnp.int32, (TILE, TILE), 1)
    return order(k) >= order(q), order(k) <= order(q)


def order_one(row):
    return (row % 8) * 16 + row // 8


def order_two(row):
    return (row % 32) * 4 + row // 32


def order_three(row):
    return row


def attend_tile(query, key, value, before, own):
    scores = lax.dot_general(
        query, key, (((1,), (1,)), ((), ())), preferred_element_type=jnp.float32
    )
    early = jnp.where(before, scores[:, :TILE], LOWEST)
    late = jnp.where(own, scores[:, TILE:], LOWEST)
    peak = jnp.max(jnp.maximum(early, late), axis=-1, keepdims=True)
    return early, late, peak, jnp.concatenate([value, jnp.ones_like(value)], axis=1)


def weigh(early, late, top, value):
    shares = jnp.concatenate(
        [jnp.exp2((early - top) * SCALE), jnp.exp2((late - top) * SCALE)], axis=1
    ).astype(jnp.bfloat16)
    both = jnp.dot(shares, value, preferred_element_type=jnp.float32)
    return both[:, :HEAD_DIM], both[:, HEAD_DIM:]


def attention_kernel(
    flag, q, k, v, k_back, v_back, out, top, total, acc, q_wide, k_wide, v_wide, natural
):
    has_back = flag[0] > 0

    for x in range(ROW_CHIPS):
        for res in range(DILATION_THREE):
            spot = (x, res // 4, res % 4)
            for source, target, shift in ((q, q_wide, 0), (k, k_wide, 1), (v, v_wide, 1)):
                rows = source[spot].astype(jnp.float32).reshape(4, 8, HEAD_DIM)
                target[4 * x + shift : 4 * x + shift + 4, res * 8 : res * 8 + 8, :] = rows
    for res in range(DILATION_THREE):
        for source, target in ((k_back, k_wide), (v_back, v_wide)):
            rows = source[3, res // 4, res % 4].astype(jnp.float32)
            target[0, res * 8 : res * 8 + 8, :] = rows[24:32]

    before, own = masks(order_one)

    def one(block, carry):
        x = block // 4
        j = pl.multiple_of((block % 4) * 8, 8)
        query = q_wide[block].astype(jnp.bfloat16)
        key = k_wide[pl.ds(block, 2)].reshape(2 * TILE, HEAD_DIM).astype(jnp.bfloat16)
        value = v_wide[pl.ds(block, 2)].reshape(2 * TILE, HEAD_DIM).astype(jnp.bfloat16)
        seen = before & ((block > 0) | has_back)
        early, late, peak, value = attend_tile(query, key, value, seen, own)
        high = jnp.broadcast_to(peak, (TILE, TILE))
        part, count = weigh(early, late, high, value)
        shape = (4, 4, 8, TILE)
        top[x, :, :, pl.ds(j, 8), :] = high.reshape(shape)
        total[x, :, :, pl.ds(j, 8), :] = count.reshape(shape)
        acc[x, :, :, pl.ds(j, 8), :] = part.reshape(shape)
        return carry

    lax.fori_loop(0, 16, one, 0)

    before, own = masks(order_two)
    for x in range(ROW_CHIPS):

        def two(res, carry, x=x):
            def rows(ref, index):
                return ref[index, :, res].reshape(TILE, HEAD_DIM)

            query = rows(q, x)
            if x == 0:
                key = jnp.concatenate([rows(k_back, 3), rows(k, 0)], axis=0)
                value = jnp.concatenate([rows(v_back, 3), rows(v, 0)], axis=0)
                seen = before & has_back
            else:
                key = jnp.concatenate([rows(k, x - 1), rows(k, x)], axis=0)
                value = jnp.concatenate([rows(v, x - 1), rows(v, x)], axis=0)
                seen = before
            early, late, peak, value = attend_tile(query, key, value, seen, own)
            old = rows(top, x)
            high = jnp.maximum(old, peak)
            part, count = weigh(early, late, high, value)
            fade = jnp.exp2((old - high) * SCALE)
            shape = (4, STEPS, TILE)
            total[x, :, res] = (rows(total, x) * fade + count).reshape(shape)
            acc[x, :, res] = (rows(acc, x) * fade + part).reshape(shape)
            top[x, :, res] = high.reshape(shape)
            return carry

        lax.fori_loop(0, DILATION_TWO, two, 0)

    before, own = masks(order_three)
    before = before & has_back

    def three(res, carry):
        def rows(ref):
            return ref[:, res // 4, res % 4].reshape(TILE, HEAD_DIM)

        key = jnp.concatenate([rows(k_back), rows(k)], axis=0)
        value = jnp.concatenate([rows(v_back), rows(v)], axis=0)
        early, late, peak, value = attend_tile(rows(q), key, value, before, own)
        old = rows(top)
        high = jnp.maximum(old, peak)
        part, count = weigh(early, late, high, value)
        fade = jnp.exp2((old - high) * SCALE)
        result = (rows(acc) * fade + part) / (rows(total) * fade + count)
        for x in range(ROW_CHIPS):
            natural[pl.ds(x * BLOCK + res, STEPS, stride=DILATION_THREE), :] = result[
                x * STEPS : (x + 1) * STEPS
            ]
        return carry

    lax.fori_loop(0, DILATION_THREE, three, 0)
    out[...] = natural[...].astype(jnp.bfloat16)


def attention(flag, q, k, v, k_back, v_back):
    split = (ROW_CHIPS, 4, 4, STEPS, HEAD_DIM)
    wide = (16, TILE, HEAD_DIM)
    return pl.pallas_call(
        attention_kernel,
        out_shape=jax.ShapeDtypeStruct((ROW_CHIPS * BLOCK, HEAD_DIM), jnp.bfloat16),
        in_specs=[SMEM] + [VMEM] * 5,
        out_specs=VMEM,
        scratch_shapes=[
            pltpu.VMEM(split, jnp.float32),
            pltpu.VMEM(split, jnp.float32),
            pltpu.VMEM(split, jnp.float32),
            pltpu.VMEM(wide, jnp.float32),
            pltpu.VMEM((17, TILE, HEAD_DIM), jnp.float32),
            pltpu.VMEM((17, TILE, HEAD_DIM), jnp.float32),
            pltpu.VMEM((ROW_CHIPS * BLOCK, HEAD_DIM), jnp.float32),
        ],
        cost_estimate=pl.CostEstimate(
            flops=2000000000, bytes_accessed=3000000, transcendentals=1600000
        ),
    )(flag, *[array.reshape(split) for array in (q, k, v, k_back, v_back)])


def first_half_kernel(place, mine, w, out):
    rows = pl.multiple_of(place[0] * BLOCK, BLOCK)
    features = jnp.concatenate([mine[head] for head in range(4)], axis=1)
    out[...] = jnp.dot(features, w[pl.ds(rows, BLOCK), :], preferred_element_type=jnp.float32)


def second_half_kernel(place, other, w, half, out):
    rows = pl.multiple_of((1 - place[0]) * BLOCK, BLOCK)
    features = jnp.concatenate([other[head] for head in range(4)], axis=1)
    product = jnp.dot(features, w[pl.ds(rows, BLOCK), :], preferred_element_type=jnp.float32)
    out[...] = (product + half[...]).astype(jnp.bfloat16)


def local(queries, keys, values, w_out):
    row = lax.axis_index("row")
    core = lax.axis_index("tp")
    rows = lax.axis_size("row")
    onward = [(i, i + 1) for i in range(rows - 1)]
    columns = w_out.shape[1]
    projection = pl.CostEstimate(
        flops=2 * BLOCK * BLOCK * columns, bytes_accessed=3000000, transcendentals=0
    )

    def across(array):
        return lax.all_to_all(array, "x", 0, 0, tiled=True)

    (k_pack,) = pack(keys)
    k = across(k_pack)
    k_back = lax.ppermute(k, "row", onward)
    v_pack, q_pack = pack(values, queries)
    v = across(v_pack)
    v_back = lax.ppermute(v, "row", onward)
    q = across(q_pack)
    flag = jnp.reshape(row, (1,)).astype(jnp.int32)
    attended = attention(flag, q, k, v, k_back, v_back)
    mine = across(attended.reshape(ROW_CHIPS, BLOCK, HEAD_DIM))
    other = lax.ppermute(mine, "tp", [(0, 1), (1, 0)])
    place = jnp.reshape(core, (1,)).astype(jnp.int32)
    half = pl.pallas_call(
        first_half_kernel,
        out_shape=jax.ShapeDtypeStruct((BLOCK, columns), jnp.float32),
        in_specs=[SMEM, VMEM, VMEM],
        out_specs=VMEM,
        cost_estimate=projection,
    )(place, mine, w_out)
    return pl.pallas_call(
        second_half_kernel,
        out_shape=jax.ShapeDtypeStruct((BLOCK, columns), jnp.bfloat16),
        in_specs=[SMEM, VMEM, VMEM, VMEM],
        out_specs=VMEM,
        cost_estimate=projection,
    )(place, other, w_out, half)


def solution(mesh):
    rows = mesh.shape["sp"] // ROW_CHIPS
    grid = Mesh(mesh.devices.reshape(rows, ROW_CHIPS, mesh.shape["tp"]), ("row", "x", "tp"))
    whole = ("row", "x")
    in_specs = (P(whole, "tp", None),) * 3 + (P(None, "tp"),)
    return jax.shard_map(
        local, mesh=grid, in_specs=in_specs, out_specs=P(whole, "tp"), check_vma=False
    )
```

```python
import math

import jax
import jax.numpy as jnp
from jax import lax
from jax.experimental import pallas as pl
from jax.experimental.pallas import tpu as pltpu
from jax.sharding import Mesh
from jax.sharding import PartitionSpec as P

DILATION_THREE = 16
HEAD_DIM = 128
ROW_CHIPS = 4
BLOCK = 512
STEPS = BLOCK // DILATION_THREE
TILE = 128
SCALE = math.log2(math.e) / math.sqrt(HEAD_DIM)
LOWEST = -1e30
KEY, VALUE, QUERY = 0, 1, 2
VMEM = pl.BlockSpec(memory_space=pltpu.VMEM)
SMEM = pl.BlockSpec(memory_space=pltpu.SMEM)
BF16 = jnp.bfloat16
F32 = jnp.float32


def room(mib):
    return pltpu.CompilerParams(vmem_limit_bytes=mib * 1024 * 1024)


def pack_kernel(place, k, v, q, row, back0, back1, back2, back3, wide_k, wide_v, wide_q):
    backs = (back0, back1, back2, back3)
    for kind, (source, wide) in enumerate(((k, wide_k), (v, wide_v), (q, wide_q))):
        wide[...] = source[...].astype(F32)
    for kind, wide in enumerate((wide_k, wide_v, wide_q)):
        for shift in range(ROW_CHIPS):
            head = (place[0] + shift) & 3
            for res in range(DILATION_THREE):
                rows = wide[pl.ds(4 * res + head, STEPS, stride=4 * DILATION_THREE), :]
                rows = rows.astype(BF16)
                row[head, kind, res * STEPS : (res + 1) * STEPS, :] = rows
                if kind != QUERY:
                    backs[shift][kind, res * STEPS : (res + 1) * STEPS, :] = rows


def pack(place, keys, values, queries):
    back = jax.ShapeDtypeStruct((2, BLOCK, HEAD_DIM), BF16)
    row = jax.ShapeDtypeStruct((ROW_CHIPS, 3, BLOCK, HEAD_DIM), BF16)
    return pl.pallas_call(
        pack_kernel,
        out_shape=[row] + [back] * 4,
        in_specs=[SMEM] + [VMEM] * 3,
        out_specs=[VMEM] * 5,
        scratch_shapes=[pltpu.VMEM((4 * BLOCK, HEAD_DIM), F32)] * 3,
        compiler_params=room(12),
        cost_estimate=pl.CostEstimate(flops=1000000, bytes_accessed=4000000, transcendentals=0),
    )(place, *[array.reshape(4 * BLOCK, HEAD_DIM) for array in (keys, values, queries)])


def order_one(row):
    return (row % 8) * 16 + row // 8


def order_two(row):
    return (row % 32) * 4 + row // 32


def order_three(row):
    return row


def set_bias(bias, order):
    q = order(lax.broadcasted_iota(jnp.int32, (TILE, TILE), 0))
    k = order(lax.broadcasted_iota(jnp.int32, (TILE, TILE), 1))
    bias[:, :TILE] = jnp.where(k >= q, 0.0, LOWEST).astype(F32)
    bias[:, TILE:] = jnp.where(k <= q, 0.0, LOWEST).astype(F32)


def product(query, key):
    return lax.dot_general(query, key, (((1,), (1,)), ((), ())), preferred_element_type=F32)


def attend(queries, keys, values, biases, olds):
    scores = [product(q, k) + bias for q, k, bias in zip(queries, keys, biases)]
    widths = [score.shape[1] // TILE for score in scores]
    peaks = []
    for score, width in zip(scores, widths):
        both = score[:, :TILE] if width == 1 else jnp.maximum(score[:, :TILE], score[:, TILE:])
        peaks.append(jnp.broadcast_to(jnp.max(both, axis=-1, keepdims=True), (TILE, TILE)))
    highs = [peak if old is None else jnp.maximum(peak, old[0]) for peak, old in zip(peaks, olds)]
    shares = []
    for score, width, high in zip(scores, widths, highs):
        parts = [
            jnp.exp2((score[:, i * TILE : (i + 1) * TILE] - high) * SCALE).astype(BF16)
            for i in range(width)
        ]
        shares.append(parts[0] if width == 1 else jnp.concatenate(parts, axis=1))
    states = []
    for share, value, high, old in zip(shares, values, highs, olds):
        both = jnp.dot(
            share,
            jnp.concatenate([value, jnp.ones_like(value)], axis=1),
            preferred_element_type=F32,
        )
        part, count = both[:, :HEAD_DIM], both[:, HEAD_DIM:]
        if old is not None:
            fade = jnp.exp2((old[0] - high) * SCALE)
            count = count + old[1] * fade
            part = part + old[2] * fade
        states.append((high, count, part))
    return states


def split_blocks(rows):
    wide = rows.astype(F32)
    return [
        wide[:, :, 8 * c : 8 * c + 8, :].reshape(TILE, HEAD_DIM).astype(BF16) for c in range(4)
    ]


def own_kernel(row, top, total, acc, q_block, k_block, v_block, bias):
    for x in range(ROW_CHIPS):
        for kind, target in ((QUERY, q_block), (KEY, k_block), (VALUE, v_block)):
            for c, block in enumerate(split_blocks(row[x, kind])):
                target[4 * x + c] = block

    set_bias(bias, order_one)
    shape = (4, 4, 8, TILE)

    def one(x):
        first = x == 0 if isinstance(x, int) else False
        queries = [q_block[4 * x + c] for c in range(4)]
        spans, biases = [], []
        for c in range(4):
            if first and c == 0:
                spans.append(pl.ds(0, 1))
                biases.append(bias[:, TILE:])
            else:
                spans.append(pl.ds(4 * x + c - 1, 2))
                biases.append(bias[...])
        keys = [k_block[span].reshape(-1, HEAD_DIM) for span in spans]
        values = [v_block[span].reshape(-1, HEAD_DIM) for span in spans]
        states = attend(queries, keys, values, biases, [None] * 4)
        for c, state in enumerate(states):
            for target, array in zip((top, total, acc), state):
                target[x, :, :, 8 * c : 8 * c + 8, :] = array.reshape(shape)

    one(0)
    lax.fori_loop(1, ROW_CHIPS, lambda x, carry: (one(x), carry)[1], 0)

    set_bias(bias, order_two)
    shape = (4, STEPS, TILE)

    def two(x):
        first = x == 0 if isinstance(x, int) else False

        def rows(kind, block, res):
            return row[block, kind, :, res].reshape(TILE, HEAD_DIM)

        def span(kind, res):
            if first:
                return rows(kind, x, res)
            return jnp.concatenate([rows(kind, x - 1, res), rows(kind, x, res)], axis=0)

        queries = [rows(QUERY, x, res) for res in range(4)]
        keys = [span(KEY, res) for res in range(4)]
        values = [span(VALUE, res) for res in range(4)]
        olds = [
            tuple(ref[x, :, res].reshape(TILE, TILE) for ref in (top, total, acc))
            for res in range(4)
        ]
        biases = [bias[:, TILE:] if first else bias[...]] * 4
        for res, state in enumerate(attend(queries, keys, values, biases, olds)):
            for target, array in zip((top, total, acc), state):
                target[x, :, res] = array.reshape(shape)

    two(0)
    lax.fori_loop(1, ROW_CHIPS, lambda x, carry: (two(x), carry)[1], 0)


def attend_own(row):
    state = jax.ShapeDtypeStruct((ROW_CHIPS, 4, 4, STEPS, HEAD_DIM), F32)
    return pl.pallas_call(
        own_kernel,
        out_shape=[state] * 3,
        in_specs=[VMEM],
        out_specs=[VMEM] * 3,
        scratch_shapes=[pltpu.VMEM((16, TILE, HEAD_DIM), BF16)] * 3
        + [pltpu.VMEM((TILE, 2 * TILE), F32)],
        compiler_params=room(16),
        cost_estimate=pl.CostEstimate(
            flops=1500000000, bytes_accessed=3000000, transcendentals=1000000
        ),
    )(row)


def back_kernel(
    place, row, back0, back1, back2, back3, top, total, acc, out,
    k_back, v_back, top0, total0, acc0, natural, bias,
):
    has_back = place[1] > 0
    for shift, back in enumerate((back0, back1, back2, back3)):
        source = (place[0] - shift) & 3
        k_back[source] = back[KEY]
        v_back[source] = back[VALUE]

    set_bias(bias, order_one)
    closed = jnp.where(has_back, 0.0, LOWEST).astype(F32)
    shape = (4, 4, 8, TILE)
    query = split_blocks(row[0, QUERY])[0]
    key = split_blocks(k_back[3])[3]
    value = split_blocks(v_back[3])[3]
    old = tuple(ref[0, :, :, 0:8, :].reshape(TILE, TILE) for ref in (top, total, acc))
    (state,) = attend([query], [key], [value], [bias[:, :TILE] + closed], [old])
    for target, source, array in zip((top0, total0, acc0), (top, total, acc), state):
        target[:, :, 0:8, :] = array.reshape(shape)
        target[:, :, 8:, :] = source[0, :, :, 8:, :]

    set_bias(bias, order_two)
    queries = [row[0, QUERY, :, res].reshape(TILE, HEAD_DIM) for res in range(4)]
    keys = [k_back[3, :, res].reshape(TILE, HEAD_DIM) for res in range(4)]
    values = [v_back[3, :, res].reshape(TILE, HEAD_DIM) for res in range(4)]
    olds = [
        tuple(ref[:, res].reshape(TILE, TILE) for ref in (top0, total0, acc0)) for res in range(4)
    ]
    states = attend(queries, keys, values, [bias[:, :TILE] + closed] * 4, olds)
    for res, state in enumerate(states):
        for target, array in zip((top0, total0, acc0), state):
            target[:, res] = array.reshape(4, STEPS, TILE)

    set_bias(bias, order_three)
    bias[:, :TILE] = bias[:, :TILE] + closed

    def three(a, carry):
        def span(ref, kind, res):
            return jnp.concatenate(
                [ref[:, a, res].reshape(TILE, HEAD_DIM), row[:, kind, a, res].reshape(TILE, HEAD_DIM)],
                axis=0,
            )

        queries = [row[:, QUERY, a, res].reshape(TILE, HEAD_DIM) for res in range(4)]
        keys = [span(k_back, KEY, res) for res in range(4)]
        values = [span(v_back, VALUE, res) for res in range(4)]
        olds = [
            tuple(
                jnp.concatenate(
                    [near[a, res], far[1:, a, res].reshape(3 * STEPS, TILE)], axis=0
                )
                for near, far in ((top0, top), (total0, total), (acc0, acc))
            )
            for res in range(4)
        ]
        states = attend(queries, keys, values, [bias[...]] * 4, olds)
        results = [part / count for _, count, part in states]
        for res, result in enumerate(results):
            for x in range(ROW_CHIPS):
                start = x * BLOCK + 4 * a + res
                natural[pl.ds(start, STEPS, stride=DILATION_THREE), :] = result[
                    x * STEPS : (x + 1) * STEPS
                ]
        return carry

    lax.fori_loop(0, 4, three, 0)
    out[...] = natural[...].astype(BF16)


def attend_back(place, row, backs, states):
    shape = (2, 4, 4, STEPS, HEAD_DIM)
    return pl.pallas_call(
        back_kernel,
        out_shape=jax.ShapeDtypeStruct((ROW_CHIPS * BLOCK, HEAD_DIM), BF16),
        in_specs=[SMEM] + [VMEM] * 8,
        out_specs=VMEM,
        scratch_shapes=[pltpu.VMEM((ROW_CHIPS, 4, 4, STEPS, HEAD_DIM), BF16)] * 2
        + [pltpu.VMEM((4, 4, STEPS, HEAD_DIM), F32)] * 3
        + [pltpu.VMEM((ROW_CHIPS * BLOCK, HEAD_DIM), F32), pltpu.VMEM((TILE, 2 * TILE), F32)],
        compiler_params=room(16),
        cost_estimate=pl.CostEstimate(
            flops=1000000000, bytes_accessed=3000000, transcendentals=600000
        ),
    )(place, row, *[back.reshape(shape) for back in backs], *states)


def first_half_kernel(place, mine, w, out):
    rows = pl.multiple_of(place[2] * BLOCK, BLOCK)
    features = jnp.concatenate([mine[head] for head in range(4)], axis=1)
    out[...] = jnp.dot(features, w[pl.ds(rows, BLOCK), :], preferred_element_type=F32)


def second_half_kernel(place, other, w, half, out):
    rows = pl.multiple_of((1 - place[2]) * BLOCK, BLOCK)
    features = jnp.concatenate([other[head] for head in range(4)], axis=1)
    rest = jnp.dot(features, w[pl.ds(rows, BLOCK), :], preferred_element_type=F32)
    out[...] = (rest + half[...]).astype(BF16)


def project(kernel, dtype, *operands):
    columns = operands[2].shape[1]
    return pl.pallas_call(
        kernel,
        out_shape=jax.ShapeDtypeStruct((BLOCK, columns), dtype),
        in_specs=[SMEM] + [VMEM] * (len(operands) - 1),
        out_specs=VMEM,
        compiler_params=room(12),
        cost_estimate=pl.CostEstimate(
            flops=2 * BLOCK * BLOCK * columns, bytes_accessed=3000000, transcendentals=0
        ),
    )(*operands)


def local(queries, keys, values, w_out):
    rows = lax.axis_size("row")
    place = jnp.stack([lax.axis_index(name) for name in ("x", "row", "tp")]).astype(jnp.int32)

    def to_next_row(array, shift):
        route = [
            (row * ROW_CHIPS + x, (row + 1) * ROW_CHIPS + (x + shift) % ROW_CHIPS)
            for row in range(rows - 1)
            for x in range(ROW_CHIPS)
        ]
        return lax.ppermute(array, ("row", "x"), route)

    row_pack, *backs = pack(place, keys, values, queries)
    backs = [to_next_row(back, shift) for shift, back in enumerate(backs)]
    row = lax.all_to_all(row_pack, "x", 0, 0, tiled=True)
    row = row.reshape(ROW_CHIPS, 3, 4, 4, STEPS, HEAD_DIM)
    states = attend_own(row)
    attended = attend_back(place, row, backs, states)
    mine = lax.all_to_all(attended.reshape(ROW_CHIPS, BLOCK, HEAD_DIM), "x", 0, 0, tiled=True)
    other = lax.ppermute(mine, "tp", [(0, 1), (1, 0)])
    half = project(first_half_kernel, F32, place, mine, w_out)
    return project(second_half_kernel, BF16, place, other, w_out, half)


def solution(mesh):
    rows = mesh.shape["sp"] // ROW_CHIPS
    grid = Mesh(mesh.devices.reshape(rows, ROW_CHIPS, mesh.shape["tp"]), ("row", "x", "tp"))
    whole = ("row", "x")
    in_specs = (P(whole, "tp", None),) * 3 + (P(None, "tp"),)
    return jax.shard_map(
        local, mesh=grid, in_specs=in_specs, out_specs=P(whole, "tp"), check_vma=False
    )
```

```python
import math

import jax
import jax.numpy as jnp
from jax import lax
from jax.experimental import pallas as pl
from jax.experimental.pallas import tpu as pltpu
from jax.sharding import Mesh
from jax.sharding import PartitionSpec as P

DILATION_THREE = 16
HEAD_DIM = 128
ROW_CHIPS = 4
BLOCK = 512
STEPS = BLOCK // DILATION_THREE
TILE = 128
GROUP = 4 * DILATION_THREE
PITCH = GROUP + 8
SCALE = math.log2(math.e) / math.sqrt(HEAD_DIM)
LOWEST = -1e30
KEY, VALUE, QUERY = 0, 1, 2
VMEM = pl.BlockSpec(memory_space=pltpu.VMEM)
SMEM = pl.BlockSpec(memory_space=pltpu.SMEM)
BF16 = jnp.bfloat16
F32 = jnp.float32


def room(mib):
    return pltpu.CompilerParams(vmem_limit_bytes=mib * 1024 * 1024)


def pack_kernel(
    place, k, v, q, row, back0, back1, back2, back3, narrow, wide, arrived
):
    backs = (back0, back1, back2, back3)
    copies = [
        pltpu.make_async_copy(source, narrow.at[kind], arrived.at[kind])
        for kind, source in enumerate((k, v, q))
    ]
    for copy in copies:
        copy.start()
    for kind, copy in enumerate(copies):
        copy.wait()
        for step in range(STEPS):
            wide[kind, step * PITCH : step * PITCH + GROUP, :] = narrow[
                kind, step * GROUP : (step + 1) * GROUP, :
            ].astype(F32)
        for shift in range(ROW_CHIPS):
            head = (place[0] + shift) & 3
            for res in range(DILATION_THREE):
                rows = wide[kind, pl.ds(4 * res + head, STEPS, stride=PITCH), :].astype(BF16)
                row[head, kind, res * STEPS : (res + 1) * STEPS, :] = rows
                if kind != QUERY:
                    backs[shift][kind, res * STEPS : (res + 1) * STEPS, :] = rows


def pack(place, keys, values, queries):
    back = jax.ShapeDtypeStruct((2, BLOCK, HEAD_DIM), BF16)
    row = jax.ShapeDtypeStruct((ROW_CHIPS, 3, BLOCK, HEAD_DIM), BF16)
    rows = 4 * BLOCK
    operands = [
        pltpu.with_memory_space_constraint(array.reshape(rows, HEAD_DIM), pltpu.HBM)
        for array in (keys, values, queries)
    ]
    return pl.pallas_call(
        pack_kernel,
        out_shape=[row] + [back] * 4,
        in_specs=[SMEM] + [pl.BlockSpec(memory_space=pltpu.HBM)] * 3,
        out_specs=[VMEM] * 5,
        scratch_shapes=[
            pltpu.VMEM((3, rows, HEAD_DIM), BF16),
            pltpu.VMEM((3, STEPS * PITCH, HEAD_DIM), F32),
            pltpu.SemaphoreType.DMA((3,)),
        ],
        compiler_params=room(14),
        cost_estimate=pl.CostEstimate(flops=1000000, bytes_accessed=4000000, transcendentals=0),
    )(place, *operands)


def order_one(row):
    return (row % 8) * 16 + row // 8


def order_two(row):
    return (row % 32) * 4 + row // 32


def order_three(row):
    return row


def set_bias(bias, order):
    q = order(lax.broadcasted_iota(jnp.int32, (TILE, TILE), 0))
    k = order(lax.broadcasted_iota(jnp.int32, (TILE, TILE), 1))
    bias[:, :TILE] = jnp.where(k >= q, 0.0, LOWEST).astype(F32)
    bias[:, TILE:] = jnp.where(k <= q, 0.0, LOWEST).astype(F32)


def product(query, key):
    return lax.dot_general(query, key, (((1,), (1,)), ((), ())), preferred_element_type=F32)


def attend(queries, keys, values, biases, olds):
    scores = [product(q, k) + bias for q, k, bias in zip(queries, keys, biases)]
    widths = [score.shape[1] // TILE for score in scores]
    peaks = []
    for score, width in zip(scores, widths):
        both = score[:, :TILE] if width == 1 else jnp.maximum(score[:, :TILE], score[:, TILE:])
        peaks.append(jnp.broadcast_to(jnp.max(both, axis=-1, keepdims=True), (TILE, TILE)))
    highs = [peak if old is None else jnp.maximum(peak, old[0]) for peak, old in zip(peaks, olds)]
    shares = []
    for score, width, high in zip(scores, widths, highs):
        parts = [
            jnp.exp2((score[:, i * TILE : (i + 1) * TILE] - high) * SCALE).astype(BF16)
            for i in range(width)
        ]
        shares.append(parts[0] if width == 1 else jnp.concatenate(parts, axis=1))
    states = []
    for share, value, high, old in zip(shares, values, highs, olds):
        both = jnp.dot(
            share,
            jnp.concatenate([value, jnp.ones_like(value)], axis=1),
            preferred_element_type=F32,
        )
        part, count = both[:, :HEAD_DIM], both[:, HEAD_DIM:]
        if old is not None:
            fade = jnp.exp2((old[0] - high) * SCALE)
            count = count + old[1] * fade
            part = part + old[2] * fade
        states.append((high, count, part))
    return states


def split_blocks(rows):
    wide = rows.astype(F32)
    return [
        wide[:, :, 8 * c : 8 * c + 8, :].reshape(TILE, HEAD_DIM).astype(BF16) for c in range(4)
    ]


def own_kernel(row, top, total, acc, q_block, k_block, v_block, bias):
    for x in range(ROW_CHIPS):
        for kind, target in ((QUERY, q_block), (KEY, k_block), (VALUE, v_block)):
            for c, block in enumerate(split_blocks(row[x, kind])):
                target[4 * x + c] = block

    set_bias(bias, order_one)
    shape = (4, 4, 8, TILE)

    def one(x):
        first = x == 0 if isinstance(x, int) else False
        queries = [q_block[4 * x + c] for c in range(4)]
        spans, biases = [], []
        for c in range(4):
            if first and c == 0:
                spans.append(pl.ds(0, 1))
                biases.append(bias[:, TILE:])
            else:
                spans.append(pl.ds(4 * x + c - 1, 2))
                biases.append(bias[...])
        keys = [k_block[span].reshape(-1, HEAD_DIM) for span in spans]
        values = [v_block[span].reshape(-1, HEAD_DIM) for span in spans]
        states = attend(queries, keys, values, biases, [None] * 4)
        for c, state in enumerate(states):
            for target, array in zip((top, total, acc), state):
                target[x, :, :, 8 * c : 8 * c + 8, :] = array.reshape(shape)

    one(0)
    for x in range(1, 4):
        one(x)

    set_bias(bias, order_two)
    shape = (4, STEPS, TILE)

    def two(x):
        first = x == 0 if isinstance(x, int) else False

        def rows(kind, block, res):
            return row[block, kind, :, res].reshape(TILE, HEAD_DIM)

        def span(kind, res):
            if first:
                return rows(kind, x, res)
            return jnp.concatenate([rows(kind, x - 1, res), rows(kind, x, res)], axis=0)

        queries = [rows(QUERY, x, res) for res in range(4)]
        keys = [span(KEY, res) for res in range(4)]
        values = [span(VALUE, res) for res in range(4)]
        olds = [
            tuple(ref[x, :, res].reshape(TILE, TILE) for ref in (top, total, acc))
            for res in range(4)
        ]
        biases = [bias[:, TILE:] if first else bias[...]] * 4
        for res, state in enumerate(attend(queries, keys, values, biases, olds)):
            for target, array in zip((top, total, acc), state):
                target[x, :, res] = array.reshape(shape)

    two(0)
    for x in range(1, 4):
        two(x)


def attend_own(row):
    state = jax.ShapeDtypeStruct((ROW_CHIPS, 4, 4, STEPS, HEAD_DIM), F32)
    return pl.pallas_call(
        own_kernel,
        out_shape=[state] * 3,
        in_specs=[VMEM],
        out_specs=[VMEM] * 3,
        scratch_shapes=[pltpu.VMEM((16, TILE, HEAD_DIM), BF16)] * 3
        + [pltpu.VMEM((TILE, 2 * TILE), F32)],
        compiler_params=room(16),
        cost_estimate=pl.CostEstimate(
            flops=1500000000, bytes_accessed=3000000, transcendentals=1000000
        ),
    )(row)


def back_kernel(
    place, row, back0, back1, back2, back3, top, total, acc, out,
    k_back, v_back, top0, total0, acc0, natural, bias,
):
    has_back = place[1] > 0
    for shift, back in enumerate((back0, back1, back2, back3)):
        source = (place[0] - shift) & 3
        k_back[source] = back[KEY]
        v_back[source] = back[VALUE]

    set_bias(bias, order_one)
    closed = jnp.where(has_back, 0.0, LOWEST).astype(F32)
    shape = (4, 4, 8, TILE)
    query = split_blocks(row[0, QUERY])[0]
    key = split_blocks(k_back[3])[3]
    value = split_blocks(v_back[3])[3]
    old = tuple(ref[0, :, :, 0:8, :].reshape(TILE, TILE) for ref in (top, total, acc))
    (state,) = attend([query], [key], [value], [bias[:, :TILE] + closed], [old])
    for target, source, array in zip((top0, total0, acc0), (top, total, acc), state):
        target[:, :, 0:8, :] = array.reshape(shape)
        target[:, :, 8:, :] = source[0, :, :, 8:, :]

    set_bias(bias, order_two)
    queries = [row[0, QUERY, :, res].reshape(TILE, HEAD_DIM) for res in range(4)]
    keys = [k_back[3, :, res].reshape(TILE, HEAD_DIM) for res in range(4)]
    values = [v_back[3, :, res].reshape(TILE, HEAD_DIM) for res in range(4)]
    olds = [
        tuple(ref[:, res].reshape(TILE, TILE) for ref in (top0, total0, acc0)) for res in range(4)
    ]
    states = attend(queries, keys, values, [bias[:, :TILE] + closed] * 4, olds)
    for res, state in enumerate(states):
        for target, array in zip((top0, total0, acc0), state):
            target[:, res] = array.reshape(4, STEPS, TILE)

    set_bias(bias, order_three)
    bias[:, :TILE] = bias[:, :TILE] + closed

    def three(a, carry):
        def span(ref, kind, res):
            return jnp.concatenate(
                [ref[:, a, res].reshape(TILE, HEAD_DIM), row[:, kind, a, res].reshape(TILE, HEAD_DIM)],
                axis=0,
            )

        queries = [row[:, QUERY, a, res].reshape(TILE, HEAD_DIM) for res in range(4)]
        keys = [span(k_back, KEY, res) for res in range(4)]
        values = [span(v_back, VALUE, res) for res in range(4)]
        olds = [
            tuple(
                jnp.concatenate(
                    [near[a, res], far[1:, a, res].reshape(3 * STEPS, TILE)], axis=0
                )
                for near, far in ((top0, top), (total0, total), (acc0, acc))
            )
            for res in range(4)
        ]
        states = attend(queries, keys, values, [bias[...]] * 4, olds)
        results = [part / count for _, count, part in states]
        for res, result in enumerate(results):
            for x in range(ROW_CHIPS):
                start = x * BLOCK + 4 * a + res
                natural[pl.ds(start, STEPS, stride=DILATION_THREE), :] = result[
                    x * STEPS : (x + 1) * STEPS
                ]
        return carry

    for a in range(4):
        three(a, 0)
    out[...] = natural[...].astype(BF16)


def attend_back(place, row, backs, states):
    shape = (2, 4, 4, STEPS, HEAD_DIM)
    return pl.pallas_call(
        back_kernel,
        out_shape=jax.ShapeDtypeStruct((ROW_CHIPS * BLOCK, HEAD_DIM), BF16),
        in_specs=[SMEM] + [VMEM] * 8,
        out_specs=VMEM,
        scratch_shapes=[pltpu.VMEM((ROW_CHIPS, 4, 4, STEPS, HEAD_DIM), BF16)] * 2
        + [pltpu.VMEM((4, 4, STEPS, HEAD_DIM), F32)] * 3
        + [pltpu.VMEM((ROW_CHIPS * BLOCK, HEAD_DIM), F32), pltpu.VMEM((TILE, 2 * TILE), F32)],
        compiler_params=room(16),
        cost_estimate=pl.CostEstimate(
            flops=1000000000, bytes_accessed=3000000, transcendentals=600000
        ),
    )(place, row, *[back.reshape(shape) for back in backs], *states)


def first_half_kernel(place, mine, w, out):
    rows = pl.multiple_of(place[2] * BLOCK, BLOCK)
    features = jnp.concatenate([mine[head] for head in range(4)], axis=1)
    out[...] = jnp.dot(features, w[pl.ds(rows, BLOCK), :], preferred_element_type=F32)


def second_half_kernel(place, other, w, half, out):
    rows = pl.multiple_of((1 - place[2]) * BLOCK, BLOCK)
    features = jnp.concatenate([other[head] for head in range(4)], axis=1)
    rest = jnp.dot(features, w[pl.ds(rows, BLOCK), :], preferred_element_type=F32)
    out[...] = (rest + half[...]).astype(BF16)


def project(kernel, dtype, *operands):
    columns = operands[2].shape[1]
    tiles = 1 if kernel is first_half_kernel else 4
    specs = [
        SMEM,
        pl.BlockSpec((4, BLOCK // tiles, HEAD_DIM), lambda i: (0, i, 0)),
        pl.BlockSpec(operands[2].shape, lambda i: (0, 0)),
        pl.BlockSpec((BLOCK // tiles, columns), lambda i: (i, 0)),
    ]
    return pl.pallas_call(
        kernel,
        grid=(tiles,),
        out_shape=jax.ShapeDtypeStruct((BLOCK, columns), dtype),
        in_specs=specs[: len(operands)],
        out_specs=specs[3],
        compiler_params=room(16),
        cost_estimate=pl.CostEstimate(
            flops=2 * BLOCK * BLOCK * columns, bytes_accessed=3000000, transcendentals=0
        ),
    )(*operands)


def local(queries, keys, values, w_out):
    rows = lax.axis_size("row")
    place = jnp.stack([lax.axis_index(name) for name in ("x", "row", "tp")]).astype(jnp.int32)

    def to_next_row(array, shift):
        route = [
            (row * ROW_CHIPS + x, (row + 1) * ROW_CHIPS + (x + shift) % ROW_CHIPS)
            for row in range(rows - 1)
            for x in range(ROW_CHIPS)
        ]
        return lax.ppermute(array, ("row", "x"), route)

    row_pack, *backs = pack(place, keys, values, queries)
    row = lax.all_to_all(row_pack, "x", 0, 0, tiled=True)
    backs = [to_next_row(back, shift) for shift, back in enumerate(backs)]
    row = row.reshape(ROW_CHIPS, 3, 4, 4, STEPS, HEAD_DIM)
    states = attend_own(row)
    attended = attend_back(place, row, backs, states)
    mine = lax.all_to_all(attended.reshape(ROW_CHIPS, BLOCK, HEAD_DIM), "x", 0, 0, tiled=True)
    other = lax.ppermute(mine, "tp", [(0, 1), (1, 0)])
    half = project(first_half_kernel, F32, place, mine, w_out)
    return project(second_half_kernel, BF16, place, other, w_out, half)


def solution(mesh):
    rows = mesh.shape["sp"] // ROW_CHIPS
    grid = Mesh(mesh.devices.reshape(rows, ROW_CHIPS, mesh.shape["tp"]), ("row", "x", "tp"))
    whole = ("row", "x")
    in_specs = (P(whole, "tp", None),) * 3 + (P(None, "tp"),)
    return jax.shard_map(
        local, mesh=grid, in_specs=in_specs, out_specs=P(whole, "tp"), check_vma=False
    )
```

```python
import math

import jax
import jax.numpy as jnp
from jax import lax
from jax.experimental import pallas as pl
from jax.experimental.pallas import tpu as pltpu
from jax.sharding import Mesh
from jax.sharding import PartitionSpec as P

DILATION_THREE = 16
HEAD_DIM = 128
ROW_CHIPS = 4
BLOCK = 512
STEPS = BLOCK // DILATION_THREE
TILE = 128
GROUP = 4 * DILATION_THREE
PITCH = GROUP + 8
SCALE = math.log2(math.e) / math.sqrt(HEAD_DIM)
LOWEST = -1e30
KEY, VALUE, QUERY = 0, 1, 2
VMEM = pl.BlockSpec(memory_space=pltpu.VMEM)
SMEM = pl.BlockSpec(memory_space=pltpu.SMEM)
BF16 = jnp.bfloat16
F32 = jnp.float32


def room(mib):
    return pltpu.CompilerParams(vmem_limit_bytes=mib * 1024 * 1024)


def pack_kernel(
    place, k, v, q, row, back0, back1, back2, back3, narrow, wide, arrived
):
    backs = (back0, back1, back2, back3)
    copies = [
        pltpu.make_async_copy(source, narrow.at[kind], arrived.at[kind])
        for kind, source in enumerate((k, v, q))
    ]
    for copy in copies:
        copy.start()
    for kind, copy in enumerate(copies):
        copy.wait()
        for step in range(STEPS):
            wide[kind, step * PITCH : step * PITCH + GROUP, :] = narrow[
                kind, step * GROUP : (step + 1) * GROUP, :
            ].astype(F32)
        for shift in range(ROW_CHIPS):
            head = (place[0] + shift) & 3
            for res in range(DILATION_THREE):
                rows = wide[kind, pl.ds(4 * res + head, STEPS, stride=PITCH), :].astype(BF16)
                row[head, kind, res * STEPS : (res + 1) * STEPS, :] = rows
                if kind != QUERY:
                    backs[shift][kind, res * STEPS : (res + 1) * STEPS, :] = rows


def pack(place, keys, values, queries):
    back = jax.ShapeDtypeStruct((2, BLOCK, HEAD_DIM), BF16)
    row = jax.ShapeDtypeStruct((ROW_CHIPS, 3, BLOCK, HEAD_DIM), BF16)
    rows = 4 * BLOCK
    operands = [
        pltpu.with_memory_space_constraint(array.reshape(rows, HEAD_DIM), pltpu.HBM)
        for array in (keys, values, queries)
    ]
    return pl.pallas_call(
        pack_kernel,
        out_shape=[row] + [back] * 4,
        in_specs=[SMEM] + [pl.BlockSpec(memory_space=pltpu.HBM)] * 3,
        out_specs=[VMEM] * 5,
        scratch_shapes=[
            pltpu.VMEM((3, rows, HEAD_DIM), BF16),
            pltpu.VMEM((3, STEPS * PITCH, HEAD_DIM), F32),
            pltpu.SemaphoreType.DMA((3,)),
        ],
        compiler_params=room(14),
        cost_estimate=pl.CostEstimate(flops=1000000, bytes_accessed=4000000, transcendentals=0),
    )(place, *operands)


def order_one(row):
    return (row % 8) * 16 + row // 8


def order_two(row):
    return (row % 32) * 4 + row // 32


def order_three(row):
    return row


def set_bias(bias, order):
    q = order(lax.broadcasted_iota(jnp.int32, (TILE, TILE), 0))
    k = order(lax.broadcasted_iota(jnp.int32, (TILE, TILE), 1))
    bias[:, :TILE] = jnp.where(k >= q, 0.0, LOWEST).astype(F32)
    bias[:, TILE:] = jnp.where(k <= q, 0.0, LOWEST).astype(F32)


def product(query, key):
    return lax.dot_general(query, key, (((1,), (1,)), ((), ())), preferred_element_type=F32)


def attend(queries, keys, values, biases, olds):
    scores = [product(q, k) + bias for q, k, bias in zip(queries, keys, biases)]
    widths = [score.shape[1] // TILE for score in scores]
    peaks = []
    for score, width in zip(scores, widths):
        both = score[:, :TILE] if width == 1 else jnp.maximum(score[:, :TILE], score[:, TILE:])
        peaks.append(jnp.broadcast_to(jnp.max(both, axis=-1, keepdims=True), (TILE, TILE)))
    highs = [peak if old is None else jnp.maximum(peak, old[0]) for peak, old in zip(peaks, olds)]
    shares = []
    for score, width, high in zip(scores, widths, highs):
        parts = [
            jnp.exp2((score[:, i * TILE : (i + 1) * TILE] - high) * SCALE).astype(BF16)
            for i in range(width)
        ]
        shares.append(parts[0] if width == 1 else jnp.concatenate(parts, axis=1))
    states = []
    for share, value, high, old in zip(shares, values, highs, olds):
        both = jnp.dot(
            share,
            jnp.concatenate([value, jnp.ones_like(value)], axis=1),
            preferred_element_type=F32,
        )
        part, count = both[:, :HEAD_DIM], both[:, HEAD_DIM:]
        if old is not None:
            fade = jnp.exp2((old[0] - high) * SCALE)
            count = count + old[1] * fade
            part = part + old[2] * fade
        states.append((high, count, part))
    return states


def split_blocks(rows):
    wide = rows.astype(F32)
    return [
        wide[:, :, 8 * c : 8 * c + 8, :].reshape(TILE, HEAD_DIM).astype(BF16) for c in range(4)
    ]


def own_kernel(row, top, total, acc, q_block, k_block, v_block, bias):
    for x in range(ROW_CHIPS):
        for kind, target in ((QUERY, q_block), (KEY, k_block), (VALUE, v_block)):
            for c, block in enumerate(split_blocks(row[x, kind])):
                target[4 * x + c] = block

    set_bias(bias, order_one)
    shape = (4, 4, 8, TILE)

    def one(x):
        first = x == 0 if isinstance(x, int) else False
        queries = [q_block[4 * x + c] for c in range(4)]
        spans, biases = [], []
        for c in range(4):
            if first and c == 0:
                spans.append(pl.ds(0, 1))
                biases.append(bias[:, TILE:])
            else:
                spans.append(pl.ds(4 * x + c - 1, 2))
                biases.append(bias[...])
        keys = [k_block[span].reshape(-1, HEAD_DIM) for span in spans]
        values = [v_block[span].reshape(-1, HEAD_DIM) for span in spans]
        states = attend(queries, keys, values, biases, [None] * 4)
        for c, state in enumerate(states):
            for target, array in zip((top, total, acc), state):
                target[x, :, :, 8 * c : 8 * c + 8, :] = array.reshape(shape)

    one(0)
    for x in range(1, 4):
        one(x)

    set_bias(bias, order_two)
    shape = (4, STEPS, TILE)

    def two(x):
        first = x == 0 if isinstance(x, int) else False

        def rows(kind, block, res):
            return row[block, kind, :, res].reshape(TILE, HEAD_DIM)

        def span(kind, res):
            if first:
                return rows(kind, x, res)
            return jnp.concatenate([rows(kind, x - 1, res), rows(kind, x, res)], axis=0)

        queries = [rows(QUERY, x, res) for res in range(4)]
        keys = [span(KEY, res) for res in range(4)]
        values = [span(VALUE, res) for res in range(4)]
        olds = [
            tuple(ref[x, :, res].reshape(TILE, TILE) for ref in (top, total, acc))
            for res in range(4)
        ]
        biases = [bias[:, TILE:] if first else bias[...]] * 4
        for res, state in enumerate(attend(queries, keys, values, biases, olds)):
            for target, array in zip((top, total, acc), state):
                target[x, :, res] = array.reshape(shape)

    two(0)
    for x in range(1, 4):
        two(x)


def attend_own(row):
    state = jax.ShapeDtypeStruct((ROW_CHIPS, 4, 4, STEPS, HEAD_DIM), F32)
    return pl.pallas_call(
        own_kernel,
        out_shape=[state] * 3,
        in_specs=[VMEM],
        out_specs=[VMEM] * 3,
        scratch_shapes=[pltpu.VMEM((16, TILE, HEAD_DIM), BF16)] * 3
        + [pltpu.VMEM((TILE, 2 * TILE), F32)],
        compiler_params=room(16),
        cost_estimate=pl.CostEstimate(
            flops=1500000000, bytes_accessed=3000000, transcendentals=1000000
        ),
    )(row)


def back_kernel(
    place, row, back0, back1, back2, back3, top, total, acc, out,
    k_back, v_back, top0, total0, acc0, natural, bias,
):
    has_back = place[1] > 0
    for shift, back in enumerate((back0, back1, back2, back3)):
        source = (place[0] - shift) & 3
        k_back[source] = back[KEY]
        v_back[source] = back[VALUE]

    set_bias(bias, order_one)
    closed = jnp.where(has_back, 0.0, LOWEST).astype(F32)
    shape = (4, 4, 8, TILE)
    query = split_blocks(row[0, QUERY])[0]
    key = split_blocks(k_back[3])[3]
    value = split_blocks(v_back[3])[3]
    old = tuple(ref[0, :, :, 0:8, :].reshape(TILE, TILE) for ref in (top, total, acc))
    (state,) = attend([query], [key], [value], [bias[:, :TILE] + closed], [old])
    for target, source, array in zip((top0, total0, acc0), (top, total, acc), state):
        target[:, :, 0:8, :] = array.reshape(shape)
        target[:, :, 8:, :] = source[0, :, :, 8:, :]

    set_bias(bias, order_two)
    queries = [row[0, QUERY, :, res].reshape(TILE, HEAD_DIM) for res in range(4)]
    keys = [k_back[3, :, res].reshape(TILE, HEAD_DIM) for res in range(4)]
    values = [v_back[3, :, res].reshape(TILE, HEAD_DIM) for res in range(4)]
    olds = [
        tuple(ref[:, res].reshape(TILE, TILE) for ref in (top0, total0, acc0)) for res in range(4)
    ]
    states = attend(queries, keys, values, [bias[:, :TILE] + closed] * 4, olds)
    for res, state in enumerate(states):
        for target, array in zip((top0, total0, acc0), state):
            target[:, res] = array.reshape(4, STEPS, TILE)

    set_bias(bias, order_three)
    bias[:, :TILE] = bias[:, :TILE] + closed

    def three(a, carry):
        def span(ref, kind, res):
            return jnp.concatenate(
                [ref[:, a, res].reshape(TILE, HEAD_DIM), row[:, kind, a, res].reshape(TILE, HEAD_DIM)],
                axis=0,
            )

        queries = [row[:, QUERY, a, res].reshape(TILE, HEAD_DIM) for res in range(4)]
        keys = [span(k_back, KEY, res) for res in range(4)]
        values = [span(v_back, VALUE, res) for res in range(4)]
        olds = [
            tuple(
                jnp.concatenate(
                    [near[a, res], far[1:, a, res].reshape(3 * STEPS, TILE)], axis=0
                )
                for near, far in ((top0, top), (total0, total), (acc0, acc))
            )
            for res in range(4)
        ]
        states = attend(queries, keys, values, [bias[...]] * 4, olds)
        results = [part / count for _, count, part in states]
        for res, result in enumerate(results):
            for x in range(ROW_CHIPS):
                start = x * BLOCK + 4 * a + res
                natural[pl.ds(start, STEPS, stride=DILATION_THREE), :] = result[
                    x * STEPS : (x + 1) * STEPS
                ]
        return carry

    for a in range(4):
        three(a, 0)
    out[...] = natural[...].astype(BF16)


def attend_back(place, row, backs, states):
    shape = (2, 4, 4, STEPS, HEAD_DIM)
    return pl.pallas_call(
        back_kernel,
        out_shape=jax.ShapeDtypeStruct((ROW_CHIPS * BLOCK, HEAD_DIM), BF16),
        in_specs=[SMEM] + [VMEM] * 8,
        out_specs=VMEM,
        scratch_shapes=[pltpu.VMEM((ROW_CHIPS, 4, 4, STEPS, HEAD_DIM), BF16)] * 2
        + [pltpu.VMEM((4, 4, STEPS, HEAD_DIM), F32)] * 3
        + [pltpu.VMEM((ROW_CHIPS * BLOCK, HEAD_DIM), F32), pltpu.VMEM((TILE, 2 * TILE), F32)],
        compiler_params=room(16),
        cost_estimate=pl.CostEstimate(
            flops=1000000000, bytes_accessed=3000000, transcendentals=600000
        ),
    )(place, row, *[back.reshape(shape) for back in backs], *states)


def first_half_kernel(place, mine, w, out):
    rows = pl.multiple_of(place[2] * BLOCK, BLOCK)
    features = jnp.concatenate([mine[head] for head in range(4)], axis=1)
    out[...] = jnp.dot(features, w[pl.ds(rows, BLOCK), :], preferred_element_type=F32)


def second_half_kernel(place, other, w, half, out, rounded, left):
    rows = pl.multiple_of((1 - place[2]) * BLOCK, BLOCK)
    part = w[pl.ds(rows, BLOCK), :]
    copies = []
    for tile in range(BLOCK // TILE):
        span = pl.ds(tile * TILE, TILE)
        features = jnp.concatenate([other[head, span] for head in range(4)], axis=1)
        rest = jnp.dot(features, part, preferred_element_type=F32)
        rounded[span, :] = (rest + half[span, :]).astype(BF16)
        copies.append(pltpu.make_async_copy(rounded.at[span], out.at[span], left.at[tile]))
        copies[-1].start()
    for copy in copies:
        copy.wait()


def project(place, features, w, half=None):
    columns = w.shape[1]
    last = half is not None
    operands = (features, w, half) if last else (features, w)
    scratch = [pltpu.VMEM((BLOCK, columns), BF16), pltpu.SemaphoreType.DMA((BLOCK // TILE,))]
    return pl.pallas_call(
        second_half_kernel if last else first_half_kernel,
        out_shape=jax.ShapeDtypeStruct((BLOCK, columns), BF16 if last else F32),
        in_specs=[SMEM] + [VMEM] * len(operands),
        out_specs=pl.BlockSpec(memory_space=pltpu.HBM) if last else VMEM,
        scratch_shapes=scratch if last else [],
        compiler_params=room(12),
        cost_estimate=pl.CostEstimate(
            flops=2 * BLOCK * BLOCK * columns, bytes_accessed=3000000, transcendentals=0
        ),
    )(place, *operands)


def local(queries, keys, values, w_out):
    rows = lax.axis_size("row")
    place = jnp.stack([lax.axis_index(name) for name in ("x", "row", "tp")]).astype(jnp.int32)

    def to_next_row(array, shift):
        route = [
            (row * ROW_CHIPS + x, (row + 1) * ROW_CHIPS + (x + shift) % ROW_CHIPS)
            for row in range(rows - 1)
            for x in range(ROW_CHIPS)
        ]
        return lax.ppermute(array, ("row", "x"), route)

    row_pack, *backs = pack(place, keys, values, queries)
    row = lax.all_to_all(row_pack, "x", 0, 0, tiled=True)
    backs = [to_next_row(back, shift) for shift, back in enumerate(backs)]
    row = row.reshape(ROW_CHIPS, 3, 4, 4, STEPS, HEAD_DIM)
    states = attend_own(row)
    attended = attend_back(place, row, backs, states)
    mine = lax.all_to_all(attended.reshape(ROW_CHIPS, BLOCK, HEAD_DIM), "x", 0, 0, tiled=True)
    other = lax.ppermute(mine, "tp", [(0, 1), (1, 0)])
    half = project(place, mine, w_out)
    return project(place, other, w_out, half)


def solution(mesh):
    rows = mesh.shape["sp"] // ROW_CHIPS
    grid = Mesh(mesh.devices.reshape(rows, ROW_CHIPS, mesh.shape["tp"]), ("row", "x", "tp"))
    whole = ("row", "x")
    in_specs = (P(whole, "tp", None),) * 3 + (P(None, "tp"),)
    return jax.shard_map(
        local, mesh=grid, in_specs=in_specs, out_specs=P(whole, "tp"), check_vma=False
    )
```

```python
import math

import jax
import jax.numpy as jnp
from jax import lax
from jax.experimental import pallas as pl
from jax.experimental.pallas import tpu as pltpu
from jax.sharding import Mesh
from jax.sharding import PartitionSpec as P

DILATION_THREE = 16
HEAD_DIM = 128
ROW_CHIPS = 4
BLOCK = 512
STEPS = BLOCK // DILATION_THREE
TILE = 128
GROUP = 4 * DILATION_THREE
PITCH = GROUP + 8
TOGETHER = ((0, 1), (2, 3))
SCALE = math.log2(math.e) / math.sqrt(HEAD_DIM)
LOWEST = -1e30
KEY, VALUE, QUERY = 0, 1, 2
VMEM = pl.BlockSpec(memory_space=pltpu.VMEM)
SMEM = pl.BlockSpec(memory_space=pltpu.SMEM)
BF16 = jnp.bfloat16
F32 = jnp.float32


def room(mib):
    return pltpu.CompilerParams(vmem_limit_bytes=mib * 1024 * 1024)


def pack_kernel(
    place, k, v, q, row, back0, back1, back2, back3, narrow, wide, arrived
):
    backs = (back0, back1, back2, back3)
    copies = [
        pltpu.make_async_copy(source, narrow.at[kind], arrived.at[kind])
        for kind, source in enumerate((k, v, q))
    ]
    for copy in copies:
        copy.start()
    for kind, copy in enumerate(copies):
        copy.wait()
        for step in range(STEPS):
            wide[kind, step * PITCH : step * PITCH + GROUP, :] = narrow[
                kind, step * GROUP : (step + 1) * GROUP, :
            ].astype(F32)
        for shift in range(ROW_CHIPS):
            head = (place[0] + shift) & 3
            for res in range(DILATION_THREE):
                rows = wide[kind, pl.ds(4 * res + head, STEPS, stride=PITCH), :].astype(BF16)
                row[head, kind, res * STEPS : (res + 1) * STEPS, :] = rows
                if kind != QUERY:
                    backs[shift][kind, res * STEPS : (res + 1) * STEPS, :] = rows


def pack(place, keys, values, queries):
    back = jax.ShapeDtypeStruct((2, BLOCK, HEAD_DIM), BF16)
    row = jax.ShapeDtypeStruct((ROW_CHIPS, 3, BLOCK, HEAD_DIM), BF16)
    rows = 4 * BLOCK
    operands = [
        pltpu.with_memory_space_constraint(array.reshape(rows, HEAD_DIM), pltpu.HBM)
        for array in (keys, values, queries)
    ]
    return pl.pallas_call(
        pack_kernel,
        out_shape=[row] + [back] * 4,
        in_specs=[SMEM] + [pl.BlockSpec(memory_space=pltpu.HBM)] * 3,
        out_specs=[VMEM] * 5,
        scratch_shapes=[
            pltpu.VMEM((3, rows, HEAD_DIM), BF16),
            pltpu.VMEM((3, STEPS * PITCH, HEAD_DIM), F32),
            pltpu.SemaphoreType.DMA((3,)),
        ],
        compiler_params=room(14),
        cost_estimate=pl.CostEstimate(flops=1000000, bytes_accessed=4000000, transcendentals=0),
    )(place, *operands)


def order_one(row):
    return (row % 8) * 16 + row // 8


def order_two(row):
    return (row % 32) * 4 + row // 32


def order_three(row):
    return row


def set_bias(bias, order):
    q = order(lax.broadcasted_iota(jnp.int32, (TILE, TILE), 0))
    k = order(lax.broadcasted_iota(jnp.int32, (TILE, TILE), 1))
    bias[:, :TILE] = jnp.where(k >= q, 0.0, LOWEST).astype(F32)
    bias[:, TILE:] = jnp.where(k <= q, 0.0, LOWEST).astype(F32)


def product(query, key):
    return lax.dot_general(query, key, (((1,), (1,)), ((), ())), preferred_element_type=F32)


def attend(queries, keys, values, biases, olds):
    scores = [product(q, k) * SCALE + bias for q, k, bias in zip(queries, keys, biases)]
    widths = [score.shape[1] // TILE for score in scores]
    peaks = []
    for score, width in zip(scores, widths):
        both = score[:, :TILE] if width == 1 else jnp.maximum(score[:, :TILE], score[:, TILE:])
        peaks.append(jnp.broadcast_to(jnp.max(both, axis=-1, keepdims=True), (TILE, TILE)))
    highs = [peak if old is None else jnp.maximum(peak, old[0]) for peak, old in zip(peaks, olds)]
    shares = []
    for score, width, high in zip(scores, widths, highs):
        parts = [
            jnp.exp2(score[:, i * TILE : (i + 1) * TILE] - high).astype(BF16)
            for i in range(width)
        ]
        shares.append(parts[0] if width == 1 else jnp.concatenate(parts, axis=1))
    states = []
    for share, value, high, old in zip(shares, values, highs, olds):
        both = jnp.dot(
            share,
            jnp.concatenate([value, jnp.ones_like(value)], axis=1),
            preferred_element_type=F32,
        )
        part, count = both[:, :HEAD_DIM], both[:, HEAD_DIM:]
        if old is not None:
            fade = jnp.exp2(old[0] - high)
            count = count + old[1] * fade
            part = part + old[2] * fade
        states.append((high, count, part))
    return states


def split_blocks(rows):
    wide = rows.astype(F32)
    return [
        wide[:, :, 8 * c : 8 * c + 8, :].reshape(TILE, HEAD_DIM).astype(BF16) for c in range(4)
    ]


def own_kernel(row, top, total, acc, q_block, k_block, v_block, bias):
    for x in range(ROW_CHIPS):
        for kind, target in ((QUERY, q_block), (KEY, k_block), (VALUE, v_block)):
            for c, block in enumerate(split_blocks(row[x, kind])):
                target[4 * x + c] = block

    set_bias(bias, order_one)
    shape = (4, 4, 8, TILE)

    for xs in TOGETHER:
        spots = [(x, c) for x in xs for c in range(4)]
        spans = [pl.ds(max(4 * x + c - 1, 0), 2 if x + c else 1) for x, c in spots]
        states = attend(
            [q_block[4 * x + c] for x, c in spots],
            [k_block[span].reshape(-1, HEAD_DIM) for span in spans],
            [v_block[span].reshape(-1, HEAD_DIM) for span in spans],
            [bias[...] if x + c else bias[:, TILE:] for x, c in spots],
            [None] * len(spots),
        )
        for (x, c), state in zip(spots, states):
            for target, array in zip((top, total, acc), state):
                target[x, :, :, 8 * c : 8 * c + 8, :] = array.reshape(shape)

    set_bias(bias, order_two)
    shape = (4, STEPS, TILE)

    def rows(kind, x, res):
        return row[x, kind, :, res].reshape(TILE, HEAD_DIM)

    def span(kind, x, res):
        late = rows(kind, x, res)
        return jnp.concatenate([rows(kind, x - 1, res), late], axis=0) if x else late

    for xs in TOGETHER:
        spots = [(x, res) for x in xs for res in range(4)]
        states = attend(
            [rows(QUERY, x, res) for x, res in spots],
            [span(KEY, x, res) for x, res in spots],
            [span(VALUE, x, res) for x, res in spots],
            [bias[...] if x else bias[:, TILE:] for x, res in spots],
            [
                tuple(ref[x, :, res].reshape(TILE, TILE) for ref in (top, total, acc))
                for x, res in spots
            ],
        )
        for (x, res), state in zip(spots, states):
            for target, array in zip((top, total, acc), state):
                target[x, :, res] = array.reshape(shape)


def attend_own(row):
    state = jax.ShapeDtypeStruct((ROW_CHIPS, 4, 4, STEPS, HEAD_DIM), F32)
    return pl.pallas_call(
        own_kernel,
        out_shape=[state] * 3,
        in_specs=[VMEM],
        out_specs=[VMEM] * 3,
        scratch_shapes=[pltpu.VMEM((16, TILE, HEAD_DIM), BF16)] * 3
        + [pltpu.VMEM((TILE, 2 * TILE), F32)],
        compiler_params=room(16),
        cost_estimate=pl.CostEstimate(
            flops=1500000000, bytes_accessed=3000000, transcendentals=1000000
        ),
    )(row)


def back_kernel(
    place, row, back0, back1, back2, back3, top, total, acc, out,
    k_back, v_back, top0, total0, acc0, natural, bias,
):
    has_back = place[1] > 0
    for shift, back in enumerate((back0, back1, back2, back3)):
        source = (place[0] - shift) & 3
        k_back[source] = back[KEY]
        v_back[source] = back[VALUE]

    set_bias(bias, order_one)
    closed = jnp.where(has_back, 0.0, LOWEST).astype(F32)
    shape = (4, 4, 8, TILE)
    query = split_blocks(row[0, QUERY])[0]
    key = split_blocks(k_back[3])[3]
    value = split_blocks(v_back[3])[3]
    old = tuple(ref[0, :, :, 0:8, :].reshape(TILE, TILE) for ref in (top, total, acc))
    (state,) = attend([query], [key], [value], [bias[:, :TILE] + closed], [old])
    for target, source, array in zip((top0, total0, acc0), (top, total, acc), state):
        target[:, :, 0:8, :] = array.reshape(shape)
        target[:, :, 8:, :] = source[0, :, :, 8:, :]

    set_bias(bias, order_two)
    queries = [row[0, QUERY, :, res].reshape(TILE, HEAD_DIM) for res in range(4)]
    keys = [k_back[3, :, res].reshape(TILE, HEAD_DIM) for res in range(4)]
    values = [v_back[3, :, res].reshape(TILE, HEAD_DIM) for res in range(4)]
    olds = [
        tuple(ref[:, res].reshape(TILE, TILE) for ref in (top0, total0, acc0)) for res in range(4)
    ]
    states = attend(queries, keys, values, [bias[:, :TILE] + closed] * 4, olds)
    for res, state in enumerate(states):
        for target, array in zip((top0, total0, acc0), state):
            target[:, res] = array.reshape(4, STEPS, TILE)

    set_bias(bias, order_three)
    bias[:, :TILE] = bias[:, :TILE] + closed

    def span(ref, kind, a, res):
        parts = (ref[:, a, res], row[:, kind, a, res])
        return jnp.concatenate([part.reshape(TILE, HEAD_DIM) for part in parts], axis=0)

    def state_of(near, far, a, res):
        rest = far[1:, a, res].reshape(3 * STEPS, TILE)
        return jnp.concatenate([near[a, res], rest], axis=0)

    for group in TOGETHER:
        spots = [(a, res) for a in group for res in range(4)]
        states = attend(
            [row[:, QUERY, a, res].reshape(TILE, HEAD_DIM) for a, res in spots],
            [span(k_back, KEY, a, res) for a, res in spots],
            [span(v_back, VALUE, a, res) for a, res in spots],
            [bias[...]] * len(spots),
            [
                tuple(
                    state_of(near, far, a, res)
                    for near, far in ((top0, top), (total0, total), (acc0, acc))
                )
                for a, res in spots
            ],
        )
        for (a, res), (_, count, part) in zip(spots, states):
            result = part / count
            for x in range(ROW_CHIPS):
                start = x * BLOCK + 4 * a + res
                natural[pl.ds(start, STEPS, stride=DILATION_THREE), :] = result[
                    x * STEPS : (x + 1) * STEPS
                ]
    out[...] = natural[...].astype(BF16)


def attend_back(place, row, backs, states):
    shape = (2, 4, 4, STEPS, HEAD_DIM)
    return pl.pallas_call(
        back_kernel,
        out_shape=jax.ShapeDtypeStruct((ROW_CHIPS * BLOCK, HEAD_DIM), BF16),
        in_specs=[SMEM] + [VMEM] * 8,
        out_specs=VMEM,
        scratch_shapes=[pltpu.VMEM((ROW_CHIPS, 4, 4, STEPS, HEAD_DIM), BF16)] * 2
        + [pltpu.VMEM((4, 4, STEPS, HEAD_DIM), F32)] * 3
        + [pltpu.VMEM((ROW_CHIPS * BLOCK, HEAD_DIM), F32), pltpu.VMEM((TILE, 2 * TILE), F32)],
        compiler_params=room(16),
        cost_estimate=pl.CostEstimate(
            flops=1000000000, bytes_accessed=3000000, transcendentals=600000
        ),
    )(place, row, *[back.reshape(shape) for back in backs], *states)


def first_half_kernel(place, mine, w, out):
    rows = pl.multiple_of(place[2] * BLOCK, BLOCK)
    features = jnp.concatenate([mine[head] for head in range(4)], axis=1)
    out[...] = jnp.dot(features, w[pl.ds(rows, BLOCK), :], preferred_element_type=F32)


def second_half_kernel(place, other, w, half, out, rounded, left):
    rows = pl.multiple_of((1 - place[2]) * BLOCK, BLOCK)
    part = w[pl.ds(rows, BLOCK), :]
    copies = []
    for tile in range(BLOCK // TILE):
        span = pl.ds(tile * TILE, TILE)
        features = jnp.concatenate([other[head, span] for head in range(4)], axis=1)
        rest = jnp.dot(features, part, preferred_element_type=F32)
        rounded[span, :] = (rest + half[span, :]).astype(BF16)
        copies.append(pltpu.make_async_copy(rounded.at[span], out.at[span], left.at[tile]))
        copies[-1].start()
    for copy in copies:
        copy.wait()


def project(place, features, w, half=None):
    columns = w.shape[1]
    last = half is not None
    operands = (features, w, half) if last else (features, w)
    scratch = [pltpu.VMEM((BLOCK, columns), BF16), pltpu.SemaphoreType.DMA((BLOCK // TILE,))]
    return pl.pallas_call(
        second_half_kernel if last else first_half_kernel,
        out_shape=jax.ShapeDtypeStruct((BLOCK, columns), BF16 if last else F32),
        in_specs=[SMEM] + [VMEM] * len(operands),
        out_specs=pl.BlockSpec(memory_space=pltpu.HBM) if last else VMEM,
        scratch_shapes=scratch if last else [],
        compiler_params=room(12),
        cost_estimate=pl.CostEstimate(
            flops=2 * BLOCK * BLOCK * columns, bytes_accessed=3000000, transcendentals=0
        ),
    )(place, *operands)


def local(queries, keys, values, w_out):
    rows = lax.axis_size("row")
    place = jnp.stack([lax.axis_index(name) for name in ("x", "row", "tp")]).astype(jnp.int32)

    def to_next_row(array, shift):
        route = [
            (row * ROW_CHIPS + x, (row + 1) * ROW_CHIPS + (x + shift) % ROW_CHIPS)
            for row in range(rows - 1)
            for x in range(ROW_CHIPS)
        ]
        return lax.ppermute(array, ("row", "x"), route)

    row_pack, *backs = pack(place, keys, values, queries)
    row = lax.all_to_all(row_pack, "x", 0, 0, tiled=True)
    backs = [to_next_row(back, shift) for shift, back in enumerate(backs)]
    row = row.reshape(ROW_CHIPS, 3, 4, 4, STEPS, HEAD_DIM)
    states = attend_own(row)
    attended = attend_back(place, row, backs, states)
    mine = lax.all_to_all(attended.reshape(ROW_CHIPS, BLOCK, HEAD_DIM), "x", 0, 0, tiled=True)
    other = lax.ppermute(mine, "tp", [(0, 1), (1, 0)])
    half = project(place, mine, w_out)
    return project(place, other, w_out, half)


def solution(mesh):
    rows = mesh.shape["sp"] // ROW_CHIPS
    grid = Mesh(mesh.devices.reshape(rows, ROW_CHIPS, mesh.shape["tp"]), ("row", "x", "tp"))
    whole = ("row", "x")
    in_specs = (P(whole, "tp", None),) * 3 + (P(None, "tp"),)
    return jax.shard_map(
        local, mesh=grid, in_specs=in_specs, out_specs=P(whole, "tp"), check_vma=False
    )
```

```python
import math

import jax
import jax.numpy as jnp
from jax import lax
from jax.experimental import pallas as pl
from jax.experimental.pallas import tpu as pltpu
from jax.sharding import Mesh
from jax.sharding import PartitionSpec as P

DILATION_THREE = 16
HEAD_DIM = 128
ROW_CHIPS = 4
BLOCK = 512
STEPS = BLOCK // DILATION_THREE
TILE = 128
GROUP = 4 * DILATION_THREE
PITCH = GROUP + 8
TOGETHER = ((0, 1), (2, 3))
SCALE = math.log2(math.e) / math.sqrt(HEAD_DIM)
LOWEST = -1e30
KEY, VALUE, QUERY = 0, 1, 2
VMEM = pl.BlockSpec(memory_space=pltpu.VMEM)
SMEM = pl.BlockSpec(memory_space=pltpu.SMEM)
BF16 = jnp.bfloat16
F32 = jnp.float32


def room(mib):
    return pltpu.CompilerParams(vmem_limit_bytes=mib * 1024 * 1024)


def pack_kernel(
    place, k, v, q, row, back0, back1, back2, back3, narrow, wide, arrived
):
    backs = (back0, back1, back2, back3)
    copies = [
        pltpu.make_async_copy(source, narrow.at[kind], arrived.at[kind])
        for kind, source in enumerate((k, v, q))
    ]
    for copy in copies:
        copy.start()
    for kind, copy in enumerate(copies):
        copy.wait()
        for step in range(STEPS):
            wide[kind, step * PITCH : step * PITCH + GROUP, :] = narrow[
                kind, step * GROUP : (step + 1) * GROUP, :
            ].astype(F32)
        for shift in range(ROW_CHIPS):
            head = (place[0] + shift) & 3
            for res in range(DILATION_THREE):
                rows = wide[kind, pl.ds(4 * res + head, STEPS, stride=PITCH), :].astype(BF16)
                row[head, kind, res * STEPS : (res + 1) * STEPS, :] = rows
                if kind != QUERY:
                    backs[shift][kind, res * STEPS : (res + 1) * STEPS, :] = rows


def pack(place, keys, values, queries):
    back = jax.ShapeDtypeStruct((2, BLOCK, HEAD_DIM), BF16)
    row = jax.ShapeDtypeStruct((ROW_CHIPS, 3, BLOCK, HEAD_DIM), BF16)
    rows = 4 * BLOCK
    operands = [
        pltpu.with_memory_space_constraint(array.reshape(rows, HEAD_DIM), pltpu.HBM)
        for array in (keys, values, queries)
    ]
    return pl.pallas_call(
        pack_kernel,
        out_shape=[row] + [back] * 4,
        in_specs=[SMEM] + [pl.BlockSpec(memory_space=pltpu.HBM)] * 3,
        out_specs=[VMEM] * 5,
        scratch_shapes=[
            pltpu.VMEM((3, rows, HEAD_DIM), BF16),
            pltpu.VMEM((3, STEPS * PITCH, HEAD_DIM), F32),
            pltpu.SemaphoreType.DMA((3,)),
        ],
        compiler_params=room(14),
        cost_estimate=pl.CostEstimate(flops=1000000, bytes_accessed=4000000, transcendentals=0),
    )(place, *operands)


def order_one(row):
    return (row % 8) * 16 + row // 8


def order_two(row):
    return (row % 32) * 4 + row // 32


def order_three(row):
    return row


def set_bias(bias, order):
    q = order(lax.broadcasted_iota(jnp.int32, (TILE, TILE), 0))
    k = order(lax.broadcasted_iota(jnp.int32, (TILE, TILE), 1))
    bias[:, :TILE] = jnp.where(k >= q, 0.0, LOWEST).astype(F32)
    bias[:, TILE:] = jnp.where(k <= q, 0.0, LOWEST).astype(F32)


def product(query, key):
    return lax.dot_general(query, key, (((1,), (1,)), ((), ())), preferred_element_type=F32)


def attend(queries, keys, values, biases, olds):
    scores = [product(q, k) * SCALE + bias for q, k, bias in zip(queries, keys, biases)]
    widths = [score.shape[1] // TILE for score in scores]
    peaks = []
    for score, width in zip(scores, widths):
        both = score[:, :TILE] if width == 1 else jnp.maximum(score[:, :TILE], score[:, TILE:])
        peaks.append(jnp.broadcast_to(jnp.max(both, axis=-1, keepdims=True), (TILE, TILE)))
    highs = [peak if old is None else jnp.maximum(peak, old[0]) for peak, old in zip(peaks, olds)]
    shares = []
    for score, width, high in zip(scores, widths, highs):
        parts = [
            jnp.exp2(score[:, i * TILE : (i + 1) * TILE] - high).astype(BF16)
            for i in range(width)
        ]
        shares.append(parts[0] if width == 1 else jnp.concatenate(parts, axis=1))
    states = []
    for share, value, high, old in zip(shares, values, highs, olds):
        both = jnp.dot(
            share,
            jnp.concatenate([value, jnp.ones_like(value)], axis=1),
            preferred_element_type=F32,
        )
        part, count = both[:, :HEAD_DIM], both[:, HEAD_DIM:]
        if old is not None:
            fade = jnp.exp2(old[0] - high)
            count = count + old[1] * fade
            part = part + old[2] * fade
        states.append((high, count, part))
    return states


def split_blocks(rows):
    wide = rows.astype(F32)
    return [
        wide[:, :, 8 * c : 8 * c + 8, :].reshape(TILE, HEAD_DIM).astype(BF16) for c in range(4)
    ]


def own_kernel(row, top, total, acc, q_block, k_block, v_block, bias):
    for x in range(ROW_CHIPS):
        for kind, target in ((QUERY, q_block), (KEY, k_block), (VALUE, v_block)):
            for c, block in enumerate(split_blocks(row[x, kind])):
                target[4 * x + c] = block

    set_bias(bias, order_one)
    shape = (4, 4, 8, TILE)

    for xs in TOGETHER:
        spots = [(x, c) for x in xs for c in range(4)]
        spans = [pl.ds(max(4 * x + c - 1, 0), 2 if x + c else 1) for x, c in spots]
        states = attend(
            [q_block[4 * x + c] for x, c in spots],
            [k_block[span].reshape(-1, HEAD_DIM) for span in spans],
            [v_block[span].reshape(-1, HEAD_DIM) for span in spans],
            [bias[...] if x + c else bias[:, TILE:] for x, c in spots],
            [None] * len(spots),
        )
        for (x, c), state in zip(spots, states):
            for target, array in zip((top, total, acc), state):
                target[x, :, :, 8 * c : 8 * c + 8, :] = array.reshape(shape)

    set_bias(bias, order_two)
    shape = (4, STEPS, TILE)

    def rows(kind, x, res):
        return row[x, kind, :, res].reshape(TILE, HEAD_DIM)

    def span(kind, x, res):
        late = rows(kind, x, res)
        return jnp.concatenate([rows(kind, x - 1, res), late], axis=0) if x else late

    for xs in TOGETHER:
        spots = [(x, res) for x in xs for res in range(4)]
        states = attend(
            [rows(QUERY, x, res) for x, res in spots],
            [span(KEY, x, res) for x, res in spots],
            [span(VALUE, x, res) for x, res in spots],
            [bias[...] if x else bias[:, TILE:] for x, res in spots],
            [
                tuple(ref[x, :, res].reshape(TILE, TILE) for ref in (top, total, acc))
                for x, res in spots
            ],
        )
        for (x, res), state in zip(spots, states):
            for target, array in zip((top, total, acc), state):
                target[x, :, res] = array.reshape(shape)


def attend_own(row):
    state = jax.ShapeDtypeStruct((ROW_CHIPS, 4, 4, STEPS, HEAD_DIM), F32)
    return pl.pallas_call(
        own_kernel,
        out_shape=[state] * 3,
        in_specs=[VMEM],
        out_specs=[VMEM] * 3,
        scratch_shapes=[pltpu.VMEM((16, TILE, HEAD_DIM), BF16)] * 3
        + [pltpu.VMEM((TILE, 2 * TILE), F32)],
        compiler_params=room(16),
        cost_estimate=pl.CostEstimate(
            flops=1500000000, bytes_accessed=3000000, transcendentals=1000000
        ),
    )(row)


def back_kernel(
    place, row, back0, back1, back2, back3, top, total, acc, out,
    k_back, v_back, top0, total0, acc0, natural, bias,
):
    has_back = place[1] > 0
    for shift, back in enumerate((back0, back1, back2, back3)):
        source = (place[0] - shift) & 3
        k_back[source] = back[KEY]
        v_back[source] = back[VALUE]

    closed = jnp.where(has_back, 0.0, LOWEST).astype(F32)
    shape = (4, 4, 8, TILE)
    set_bias(bias, order_one)
    bias_one = bias[:, :TILE] + closed
    set_bias(bias, order_two)
    bias_two = bias[:, :TILE] + closed
    old = tuple(ref[0, :, :, 0:8, :].reshape(TILE, TILE) for ref in (top, total, acc))
    state, *states = attend(
        [split_blocks(row[0, QUERY])[0]]
        + [row[0, QUERY, :, res].reshape(TILE, HEAD_DIM) for res in range(4)],
        [split_blocks(k_back[3])[3]]
        + [k_back[3, :, res].reshape(TILE, HEAD_DIM) for res in range(4)],
        [split_blocks(v_back[3])[3]]
        + [v_back[3, :, res].reshape(TILE, HEAD_DIM) for res in range(4)],
        [bias_one] + [bias_two] * 4,
        [old] + [None] * 4,
    )
    for target, source, array in zip((top0, total0, acc0), (top, total, acc), state):
        target[:, :, 0:8, :] = array.reshape(shape)
        target[:, :, 8:, :] = source[0, :, :, 8:, :]
    olds = [
        tuple(ref[:, res].reshape(TILE, TILE) for ref in (top0, total0, acc0)) for res in range(4)
    ]
    for res, (new, old) in enumerate(zip(states, olds)):
        high = jnp.maximum(new[0], old[0])
        fade_new, fade_old = jnp.exp2(new[0] - high), jnp.exp2(old[0] - high)
        merged = [high] + [n * fade_new + o * fade_old for n, o in zip(new[1:], old[1:])]
        for target, array in zip((top0, total0, acc0), merged):
            target[:, res] = array.reshape(4, STEPS, TILE)

    set_bias(bias, order_three)
    bias[:, :TILE] = bias[:, :TILE] + closed

    def span(ref, kind, a, res):
        parts = (ref[:, a, res], row[:, kind, a, res])
        return jnp.concatenate([part.reshape(TILE, HEAD_DIM) for part in parts], axis=0)

    def state_of(near, far, a, res):
        rest = far[1:, a, res].reshape(3 * STEPS, TILE)
        return jnp.concatenate([near[a, res], rest], axis=0)

    for group in TOGETHER:
        spots = [(a, res) for a in group for res in range(4)]
        states = attend(
            [row[:, QUERY, a, res].reshape(TILE, HEAD_DIM) for a, res in spots],
            [span(k_back, KEY, a, res) for a, res in spots],
            [span(v_back, VALUE, a, res) for a, res in spots],
            [bias[...]] * len(spots),
            [
                tuple(
                    state_of(near, far, a, res)
                    for near, far in ((top0, top), (total0, total), (acc0, acc))
                )
                for a, res in spots
            ],
        )
        for (a, res), (_, count, part) in zip(spots, states):
            result = part / count
            for x in range(ROW_CHIPS):
                start = x * BLOCK + 4 * a + res
                natural[pl.ds(start, STEPS, stride=DILATION_THREE), :] = result[
                    x * STEPS : (x + 1) * STEPS
                ]
    out[...] = natural[...].astype(BF16)


def attend_back(place, row, backs, states):
    shape = (2, 4, 4, STEPS, HEAD_DIM)
    return pl.pallas_call(
        back_kernel,
        out_shape=jax.ShapeDtypeStruct((ROW_CHIPS * BLOCK, HEAD_DIM), BF16),
        in_specs=[SMEM] + [VMEM] * 8,
        out_specs=VMEM,
        scratch_shapes=[pltpu.VMEM((ROW_CHIPS, 4, 4, STEPS, HEAD_DIM), BF16)] * 2
        + [pltpu.VMEM((4, 4, STEPS, HEAD_DIM), F32)] * 3
        + [pltpu.VMEM((ROW_CHIPS * BLOCK, HEAD_DIM), F32), pltpu.VMEM((TILE, 2 * TILE), F32)],
        compiler_params=room(16),
        cost_estimate=pl.CostEstimate(
            flops=1000000000, bytes_accessed=3000000, transcendentals=600000
        ),
    )(place, row, *[back.reshape(shape) for back in backs], *states)


def first_half_kernel(place, mine, w, out):
    rows = pl.multiple_of(place[2] * BLOCK, BLOCK)
    features = jnp.concatenate([mine[head] for head in range(4)], axis=1)
    out[...] = jnp.dot(features, w[pl.ds(rows, BLOCK), :], preferred_element_type=F32)


def second_half_kernel(place, other, w, half, out, rounded, left):
    rows = pl.multiple_of((1 - place[2]) * BLOCK, BLOCK)
    part = w[pl.ds(rows, BLOCK), :]
    copies = []
    for tile in range(BLOCK // TILE):
        span = pl.ds(tile * TILE, TILE)
        features = jnp.concatenate([other[head, span] for head in range(4)], axis=1)
        rest = jnp.dot(features, part, preferred_element_type=F32)
        rounded[span, :] = (rest + half[span, :]).astype(BF16)
        copies.append(pltpu.make_async_copy(rounded.at[span], out.at[span], left.at[tile]))
        copies[-1].start()
    for copy in copies:
        copy.wait()


def project(place, features, w, half=None):
    columns = w.shape[1]
    last = half is not None
    operands = (features, w, half) if last else (features, w)
    scratch = [pltpu.VMEM((BLOCK, columns), BF16), pltpu.SemaphoreType.DMA((BLOCK // TILE,))]
    return pl.pallas_call(
        second_half_kernel if last else first_half_kernel,
        out_shape=jax.ShapeDtypeStruct((BLOCK, columns), BF16 if last else F32),
        in_specs=[SMEM] + [VMEM] * len(operands),
        out_specs=pl.BlockSpec(memory_space=pltpu.HBM) if last else VMEM,
        scratch_shapes=scratch if last else [],
        compiler_params=room(12),
        cost_estimate=pl.CostEstimate(
            flops=2 * BLOCK * BLOCK * columns, bytes_accessed=3000000, transcendentals=0
        ),
    )(place, *operands)


def local(queries, keys, values, w_out):
    rows = lax.axis_size("row")
    place = jnp.stack([lax.axis_index(name) for name in ("x", "row", "tp")]).astype(jnp.int32)

    def to_next_row(array, shift):
        route = [
            (row * ROW_CHIPS + x, (row + 1) * ROW_CHIPS + (x + shift) % ROW_CHIPS)
            for row in range(rows - 1)
            for x in range(ROW_CHIPS)
        ]
        return lax.ppermute(array, ("row", "x"), route)

    row_pack, *backs = pack(place, keys, values, queries)
    row = lax.all_to_all(row_pack, "x", 0, 0, tiled=True)
    backs = [to_next_row(back, shift) for shift, back in enumerate(backs)]
    row = row.reshape(ROW_CHIPS, 3, 4, 4, STEPS, HEAD_DIM)
    states = attend_own(row)
    attended = attend_back(place, row, backs, states)
    mine = lax.all_to_all(attended.reshape(ROW_CHIPS, BLOCK, HEAD_DIM), "x", 0, 0, tiled=True)
    other = lax.ppermute(mine, "tp", [(0, 1), (1, 0)])
    half = project(place, mine, w_out)
    return project(place, other, w_out, half)


def solution(mesh):
    rows = mesh.shape["sp"] // ROW_CHIPS
    grid = Mesh(mesh.devices.reshape(rows, ROW_CHIPS, mesh.shape["tp"]), ("row", "x", "tp"))
    whole = ("row", "x")
    in_specs = (P(whole, "tp", None),) * 3 + (P(None, "tp"),)
    return jax.shard_map(
        local, mesh=grid, in_specs=in_specs, out_specs=P(whole, "tp"), check_vma=False
    )
```

```python
import math

import jax
import jax.numpy as jnp
from jax import lax
from jax.experimental import pallas as pl
from jax.experimental.pallas import tpu as pltpu
from jax.sharding import Mesh
from jax.sharding import PartitionSpec as P

DILATION_THREE = 16
HEAD_DIM = 128
ROW_CHIPS = 4
BLOCK = 512
STEPS = BLOCK // DILATION_THREE
TILE = 128
SLAB = 256
GROUP = 4 * DILATION_THREE
PITCH = GROUP + 8
TOGETHER = ((0, 1), (2, 3))
SCALE = math.log2(math.e) / math.sqrt(HEAD_DIM)
LOWEST = -1e30
KEY, VALUE, QUERY = 0, 1, 2
VMEM = pl.BlockSpec(memory_space=pltpu.VMEM)
SMEM = pl.BlockSpec(memory_space=pltpu.SMEM)
BF16 = jnp.bfloat16
F32 = jnp.float32


def room(mib):
    return pltpu.CompilerParams(vmem_limit_bytes=mib * 1024 * 1024)


def pack_kernel(
    place, k, v, q, row, back0, back1, back2, back3, narrow, wide, arrived
):
    backs = (back0, back1, back2, back3)
    copies = [
        pltpu.make_async_copy(source, narrow.at[kind], arrived.at[kind])
        for kind, source in enumerate((k, v, q))
    ]
    for copy in copies:
        copy.start()
    for kind, copy in enumerate(copies):
        copy.wait()
        for step in range(STEPS):
            wide[kind, step * PITCH : step * PITCH + GROUP, :] = narrow[
                kind, step * GROUP : (step + 1) * GROUP, :
            ].astype(F32)
        for shift in range(ROW_CHIPS):
            head = (place[0] + shift) & 3
            for res in range(DILATION_THREE):
                rows = wide[kind, pl.ds(4 * res + head, STEPS, stride=PITCH), :].astype(BF16)
                row[head, kind, res * STEPS : (res + 1) * STEPS, :] = rows
                if kind != QUERY:
                    backs[shift][kind, res * STEPS : (res + 1) * STEPS, :] = rows


def pack(place, keys, values, queries):
    back = jax.ShapeDtypeStruct((2, BLOCK, HEAD_DIM), BF16)
    row = jax.ShapeDtypeStruct((ROW_CHIPS, 3, BLOCK, HEAD_DIM), BF16)
    rows = 4 * BLOCK
    operands = [
        pltpu.with_memory_space_constraint(array.reshape(rows, HEAD_DIM), pltpu.HBM)
        for array in (keys, values, queries)
    ]
    return pl.pallas_call(
        pack_kernel,
        out_shape=[row] + [back] * 4,
        in_specs=[SMEM] + [pl.BlockSpec(memory_space=pltpu.HBM)] * 3,
        out_specs=[VMEM] * 5,
        scratch_shapes=[
            pltpu.VMEM((3, rows, HEAD_DIM), BF16),
            pltpu.VMEM((3, STEPS * PITCH, HEAD_DIM), F32),
            pltpu.SemaphoreType.DMA((3,)),
        ],
        compiler_params=room(14),
        cost_estimate=pl.CostEstimate(flops=1000000, bytes_accessed=4000000, transcendentals=0),
    )(place, *operands)


def order_one(row):
    return (row % 8) * 16 + row // 8


def order_two(row):
    return (row % 32) * 4 + row // 32


def order_three(row):
    return row


def set_bias(bias, order):
    q = order(lax.broadcasted_iota(jnp.int32, (TILE, TILE), 0))
    k = order(lax.broadcasted_iota(jnp.int32, (TILE, TILE), 1))
    bias[:, :TILE] = jnp.where(k >= q, 0.0, LOWEST).astype(F32)
    bias[:, TILE:] = jnp.where(k <= q, 0.0, LOWEST).astype(F32)


def product(query, key):
    return lax.dot_general(query, key, (((1,), (1,)), ((), ())), preferred_element_type=F32)


def attend(queries, keys, values, biases, olds):
    scores = [product(q, k) * SCALE + bias for q, k, bias in zip(queries, keys, biases)]
    widths = [score.shape[1] // TILE for score in scores]
    peaks = []
    for score, width in zip(scores, widths):
        both = score[:, :TILE] if width == 1 else jnp.maximum(score[:, :TILE], score[:, TILE:])
        peaks.append(jnp.broadcast_to(jnp.max(both, axis=-1, keepdims=True), (TILE, TILE)))
    highs = [peak if old is None else jnp.maximum(peak, old[0]) for peak, old in zip(peaks, olds)]
    shares = []
    for score, width, high in zip(scores, widths, highs):
        parts = [
            jnp.exp2(score[:, i * TILE : (i + 1) * TILE] - high).astype(BF16)
            for i in range(width)
        ]
        shares.append(parts[0] if width == 1 else jnp.concatenate(parts, axis=1))
    states = []
    for share, value, high, old in zip(shares, values, highs, olds):
        both = jnp.dot(
            share,
            jnp.concatenate([value, jnp.ones_like(value)], axis=1),
            preferred_element_type=F32,
        )
        part, count = both[:, :HEAD_DIM], both[:, HEAD_DIM:]
        if old is not None:
            fade = jnp.exp2(old[0] - high)
            count = count + old[1] * fade
            part = part + old[2] * fade
        states.append((high, count, part))
    return states


def split_blocks(rows):
    wide = rows.astype(F32)
    return [
        wide[:, :, 8 * c : 8 * c + 8, :].reshape(TILE, HEAD_DIM).astype(BF16) for c in range(4)
    ]


def own_kernel(row, top, total, acc, q_block, k_block, v_block, bias):
    for x in range(ROW_CHIPS):
        for kind, target in ((QUERY, q_block), (KEY, k_block), (VALUE, v_block)):
            for c, block in enumerate(split_blocks(row[x, kind])):
                target[4 * x + c] = block

    set_bias(bias, order_one)
    shape = (4, 4, 8, TILE)

    for xs in TOGETHER:
        spots = [(x, c) for x in xs for c in range(4)]
        spans = [pl.ds(max(4 * x + c - 1, 0), 2 if x + c else 1) for x, c in spots]
        states = attend(
            [q_block[4 * x + c] for x, c in spots],
            [k_block[span].reshape(-1, HEAD_DIM) for span in spans],
            [v_block[span].reshape(-1, HEAD_DIM) for span in spans],
            [bias[...] if x + c else bias[:, TILE:] for x, c in spots],
            [None] * len(spots),
        )
        for (x, c), state in zip(spots, states):
            for target, array in zip((top, total, acc), state):
                target[x, :, :, 8 * c : 8 * c + 8, :] = array.reshape(shape)

    set_bias(bias, order_two)
    shape = (4, STEPS, TILE)

    def rows(kind, x, res):
        return row[x, kind, :, res].reshape(TILE, HEAD_DIM)

    def span(kind, x, res):
        late = rows(kind, x, res)
        return jnp.concatenate([rows(kind, x - 1, res), late], axis=0) if x else late

    for xs in TOGETHER:
        spots = [(x, res) for x in xs for res in range(4)]
        states = attend(
            [rows(QUERY, x, res) for x, res in spots],
            [span(KEY, x, res) for x, res in spots],
            [span(VALUE, x, res) for x, res in spots],
            [bias[...] if x else bias[:, TILE:] for x, res in spots],
            [
                tuple(ref[x, :, res].reshape(TILE, TILE) for ref in (top, total, acc))
                for x, res in spots
            ],
        )
        for (x, res), state in zip(spots, states):
            for target, array in zip((top, total, acc), state):
                target[x, :, res] = array.reshape(shape)


def attend_own(row):
    state = jax.ShapeDtypeStruct((ROW_CHIPS, 4, 4, STEPS, HEAD_DIM), F32)
    return pl.pallas_call(
        own_kernel,
        out_shape=[state] * 3,
        in_specs=[VMEM],
        out_specs=[VMEM] * 3,
        scratch_shapes=[pltpu.VMEM((16, TILE, HEAD_DIM), BF16)] * 3
        + [pltpu.VMEM((TILE, 2 * TILE), F32)],
        compiler_params=room(16),
        cost_estimate=pl.CostEstimate(
            flops=1500000000, bytes_accessed=3000000, transcendentals=1000000
        ),
    )(row)


def back_kernel(
    place, row, back0, back1, back2, back3, top, total, acc, out,
    k_back, v_back, top0, total0, acc0, natural, bias,
):
    has_back = place[1] > 0
    for shift, back in enumerate((back0, back1, back2, back3)):
        source = (place[0] - shift) & 3
        k_back[source] = back[KEY]
        v_back[source] = back[VALUE]

    closed = jnp.where(has_back, 0.0, LOWEST).astype(F32)
    shape = (4, 4, 8, TILE)
    set_bias(bias, order_one)
    bias_one = bias[:, :TILE] + closed
    set_bias(bias, order_two)
    bias_two = bias[:, :TILE] + closed
    old = tuple(ref[0, :, :, 0:8, :].reshape(TILE, TILE) for ref in (top, total, acc))
    state, *states = attend(
        [split_blocks(row[0, QUERY])[0]]
        + [row[0, QUERY, :, res].reshape(TILE, HEAD_DIM) for res in range(4)],
        [split_blocks(k_back[3])[3]]
        + [k_back[3, :, res].reshape(TILE, HEAD_DIM) for res in range(4)],
        [split_blocks(v_back[3])[3]]
        + [v_back[3, :, res].reshape(TILE, HEAD_DIM) for res in range(4)],
        [bias_one] + [bias_two] * 4,
        [old] + [None] * 4,
    )
    for target, source, array in zip((top0, total0, acc0), (top, total, acc), state):
        target[:, :, 0:8, :] = array.reshape(shape)
        target[:, :, 8:, :] = source[0, :, :, 8:, :]
    olds = [
        tuple(ref[:, res].reshape(TILE, TILE) for ref in (top0, total0, acc0)) for res in range(4)
    ]
    for res, (new, old) in enumerate(zip(states, olds)):
        high = jnp.maximum(new[0], old[0])
        fade_new, fade_old = jnp.exp2(new[0] - high), jnp.exp2(old[0] - high)
        merged = [high] + [n * fade_new + o * fade_old for n, o in zip(new[1:], old[1:])]
        for target, array in zip((top0, total0, acc0), merged):
            target[:, res] = array.reshape(4, STEPS, TILE)

    set_bias(bias, order_three)
    bias[:, :TILE] = bias[:, :TILE] + closed

    def span(ref, kind, a, res):
        parts = (ref[:, a, res], row[:, kind, a, res])
        return jnp.concatenate([part.reshape(TILE, HEAD_DIM) for part in parts], axis=0)

    def state_of(near, far, a, res):
        rest = far[1:, a, res].reshape(3 * STEPS, TILE)
        return jnp.concatenate([near[a, res], rest], axis=0)

    for group in TOGETHER:
        spots = [(a, res) for a in group for res in range(4)]
        states = attend(
            [row[:, QUERY, a, res].reshape(TILE, HEAD_DIM) for a, res in spots],
            [span(k_back, KEY, a, res) for a, res in spots],
            [span(v_back, VALUE, a, res) for a, res in spots],
            [bias[...]] * len(spots),
            [
                tuple(
                    state_of(near, far, a, res)
                    for near, far in ((top0, top), (total0, total), (acc0, acc))
                )
                for a, res in spots
            ],
        )
        for (a, res), (_, count, part) in zip(spots, states):
            result = part / count
            for x in range(ROW_CHIPS):
                start = x * BLOCK + 4 * a + res
                natural[pl.ds(start, STEPS, stride=DILATION_THREE), :] = result[
                    x * STEPS : (x + 1) * STEPS
                ]
    out[...] = natural[...].astype(BF16)


def attend_back(place, row, backs, states):
    shape = (2, 4, 4, STEPS, HEAD_DIM)
    return pl.pallas_call(
        back_kernel,
        out_shape=jax.ShapeDtypeStruct((ROW_CHIPS * BLOCK, HEAD_DIM), BF16),
        in_specs=[SMEM] + [VMEM] * 8,
        out_specs=VMEM,
        scratch_shapes=[pltpu.VMEM((ROW_CHIPS, 4, 4, STEPS, HEAD_DIM), BF16)] * 2
        + [pltpu.VMEM((4, 4, STEPS, HEAD_DIM), F32)] * 3
        + [pltpu.VMEM((ROW_CHIPS * BLOCK, HEAD_DIM), F32), pltpu.VMEM((TILE, 2 * TILE), F32)],
        compiler_params=room(16),
        cost_estimate=pl.CostEstimate(
            flops=1000000000, bytes_accessed=3000000, transcendentals=600000
        ),
    )(place, row, *[back.reshape(shape) for back in backs], *states)


def first_half_kernel(place, mine, w, out):
    rows = pl.multiple_of(place[2] * BLOCK, BLOCK)
    features = jnp.concatenate([mine[head] for head in range(4)], axis=1)
    out[...] = jnp.dot(features, w[pl.ds(rows, BLOCK), :], preferred_element_type=F32)


def second_half_kernel(place, other, w, half, out, rounded, left):
    rows = pl.multiple_of((1 - place[2]) * BLOCK, BLOCK)
    part = w[pl.ds(rows, BLOCK), :]
    copies = []
    for tile in range(BLOCK // SLAB):
        span = pl.ds(tile * SLAB, SLAB)
        features = jnp.concatenate([other[head, span] for head in range(4)], axis=1)
        rest = jnp.dot(features, part, preferred_element_type=F32)
        rounded[span, :] = (rest + half[span, :]).astype(BF16)
        copies.append(pltpu.make_async_copy(rounded.at[span], out.at[span], left.at[tile]))
        copies[-1].start()
    for copy in copies:
        copy.wait()


def project(place, features, w, half=None):
    columns = w.shape[1]
    last = half is not None
    operands = (features, w, half) if last else (features, w)
    scratch = [pltpu.VMEM((BLOCK, columns), BF16), pltpu.SemaphoreType.DMA((BLOCK // SLAB,))]
    return pl.pallas_call(
        second_half_kernel if last else first_half_kernel,
        out_shape=jax.ShapeDtypeStruct((BLOCK, columns), BF16 if last else F32),
        in_specs=[SMEM] + [VMEM] * len(operands),
        out_specs=pl.BlockSpec(memory_space=pltpu.HBM) if last else VMEM,
        scratch_shapes=scratch if last else [],
        compiler_params=room(12),
        cost_estimate=pl.CostEstimate(
            flops=2 * BLOCK * BLOCK * columns, bytes_accessed=3000000, transcendentals=0
        ),
    )(place, *operands)


def local(queries, keys, values, w_out):
    rows = lax.axis_size("row")
    place = jnp.stack([lax.axis_index(name) for name in ("x", "row", "tp")]).astype(jnp.int32)

    def to_next_row(array, shift):
        route = [
            (row * ROW_CHIPS + x, (row + 1) * ROW_CHIPS + (x + shift) % ROW_CHIPS)
            for row in range(rows - 1)
            for x in range(ROW_CHIPS)
        ]
        return lax.ppermute(array, ("row", "x"), route)

    row_pack, *backs = pack(place, keys, values, queries)
    row = lax.all_to_all(row_pack, "x", 0, 0, tiled=True)
    back0, back1, back2, back3 = backs
    back0, back1, back3 = to_next_row(back0, 0), to_next_row(back1, 1), to_next_row(back3, 3)
    back0, back2 = lax.optimization_barrier((back0, back2))
    backs = [back0, back1, to_next_row(back2, 2), back3]
    row = row.reshape(ROW_CHIPS, 3, 4, 4, STEPS, HEAD_DIM)
    states = attend_own(row)
    attended = attend_back(place, row, backs, states)
    mine = lax.all_to_all(attended.reshape(ROW_CHIPS, BLOCK, HEAD_DIM), "x", 0, 0, tiled=True)
    other = lax.ppermute(mine, "tp", [(0, 1), (1, 0)])
    half = project(place, mine, w_out)
    return project(place, other, w_out, half)


def solution(mesh):
    rows = mesh.shape["sp"] // ROW_CHIPS
    grid = Mesh(mesh.devices.reshape(rows, ROW_CHIPS, mesh.shape["tp"]), ("row", "x", "tp"))
    whole = ("row", "x")
    in_specs = (P(whole, "tp", None),) * 3 + (P(None, "tp"),)
    return jax.shard_map(
        local, mesh=grid, in_specs=in_specs, out_specs=P(whole, "tp"), check_vma=False
    )
```

```python
import math

import jax
import jax.numpy as jnp
from jax import lax
from jax.experimental import pallas as pl
from jax.experimental.pallas import tpu as pltpu
from jax.sharding import Mesh
from jax.sharding import PartitionSpec as P

DILATION_THREE = 16
HEAD_DIM = 128
ROW_CHIPS = 4
BLOCK = 512
STEPS = BLOCK // DILATION_THREE
TILE = 128
GROUP = 4 * DILATION_THREE
PITCH = GROUP + 1
TOGETHER = ((0, 1), (2, 3))
SCALE = math.log2(math.e) / math.sqrt(HEAD_DIM)
LOWEST = -1e30
KEY, VALUE, QUERY = 0, 1, 2
VMEM = pl.BlockSpec(memory_space=pltpu.VMEM)
SMEM = pl.BlockSpec(memory_space=pltpu.SMEM)
BF16 = jnp.bfloat16
F32 = jnp.float32


def room(mib):
    return pltpu.CompilerParams(vmem_limit_bytes=mib * 1024 * 1024)


def pack_kernel(
    place, k, v, q, row, back0, back1, back2, back3, narrow, wide, arrived
):
    backs = (back0, back1, back2, back3)
    copies = [
        pltpu.make_async_copy(source, narrow.at[kind], arrived.at[kind])
        for kind, source in enumerate((k, v, q))
    ]
    for copy in copies:
        copy.start()
    for kind, copy in enumerate(copies):
        copy.wait()
        for step in range(STEPS):
            wide[kind, step * PITCH : step * PITCH + GROUP, :] = narrow[
                kind, step * GROUP : (step + 1) * GROUP, :
            ].astype(F32)
        for shift in range(ROW_CHIPS):
            head = (place[0] + shift) & 3
            for res in range(DILATION_THREE):
                rows = wide[kind, pl.ds(4 * res + head, STEPS, stride=PITCH), :].astype(BF16)
                row[head, kind, res * STEPS : (res + 1) * STEPS, :] = rows
                if kind != QUERY:
                    backs[shift][kind, res * STEPS : (res + 1) * STEPS, :] = rows


def pack(place, keys, values, queries):
    back = jax.ShapeDtypeStruct((2, BLOCK, HEAD_DIM), BF16)
    row = jax.ShapeDtypeStruct((ROW_CHIPS, 3, BLOCK, HEAD_DIM), BF16)
    rows = 4 * BLOCK
    operands = [
        pltpu.with_memory_space_constraint(array.reshape(rows, HEAD_DIM), pltpu.HBM)
        for array in (keys, values, queries)
    ]
    return pl.pallas_call(
        pack_kernel,
        out_shape=[row] + [back] * 4,
        in_specs=[SMEM] + [pl.BlockSpec(memory_space=pltpu.HBM)] * 3,
        out_specs=[VMEM] * 5,
        scratch_shapes=[
            pltpu.VMEM((3, rows, HEAD_DIM), BF16),
            pltpu.VMEM((3, STEPS * PITCH, HEAD_DIM), F32),
            pltpu.SemaphoreType.DMA((3,)),
        ],
        compiler_params=room(14),
        cost_estimate=pl.CostEstimate(flops=1000000, bytes_accessed=4000000, transcendentals=0),
    )(place, *operands)


def order_one(row):
    return (row % 8) * 16 + row // 8


def order_two(row):
    return (row % 32) * 4 + row // 32


def order_three(row):
    return row


def set_bias(bias, order):
    q = order(lax.broadcasted_iota(jnp.int32, (TILE, TILE), 0))
    k = order(lax.broadcasted_iota(jnp.int32, (TILE, TILE), 1))
    bias[:, :TILE] = jnp.where(k >= q, 0.0, LOWEST).astype(F32)
    bias[:, TILE:] = jnp.where(k <= q, 0.0, LOWEST).astype(F32)


def product(query, key):
    return lax.dot_general(query, key, (((1,), (1,)), ((), ())), preferred_element_type=F32)


def attend(queries, keys, values, biases, olds):
    scores = [product(q, k) * SCALE + bias for q, k, bias in zip(queries, keys, biases)]
    widths = [score.shape[1] // TILE for score in scores]
    peaks = []
    for score, width in zip(scores, widths):
        both = score[:, :TILE] if width == 1 else jnp.maximum(score[:, :TILE], score[:, TILE:])
        peaks.append(jnp.broadcast_to(jnp.max(both, axis=-1, keepdims=True), (TILE, TILE)))
    highs = [peak if old is None else jnp.maximum(peak, old[0]) for peak, old in zip(peaks, olds)]
    shares = []
    for score, width, high in zip(scores, widths, highs):
        parts = [
            jnp.exp2(score[:, i * TILE : (i + 1) * TILE] - high).astype(BF16)
            for i in range(width)
        ]
        shares.append(parts[0] if width == 1 else jnp.concatenate(parts, axis=1))
    states = []
    for share, value, high, old in zip(shares, values, highs, olds):
        both = jnp.dot(
            share,
            jnp.concatenate([value, jnp.ones_like(value)], axis=1),
            preferred_element_type=F32,
        )
        part, count = both[:, :HEAD_DIM], both[:, HEAD_DIM:]
        if old is not None:
            fade = jnp.exp2(old[0] - high)
            count = count + old[1] * fade
            part = part + old[2] * fade
        states.append((high, count, part))
    return states


def split_blocks(rows):
    wide = rows.astype(F32)
    return [
        wide[:, :, 8 * c : 8 * c + 8, :].reshape(TILE, HEAD_DIM).astype(BF16) for c in range(4)
    ]


def own_kernel(row, top, total, acc, q_block, k_block, v_block, bias):
    for x in range(ROW_CHIPS):
        for kind, target in ((QUERY, q_block), (KEY, k_block), (VALUE, v_block)):
            for c, block in enumerate(split_blocks(row[x, kind])):
                target[4 * x + c] = block

    set_bias(bias, order_one)
    shape = (4, 4, 8, TILE)

    for xs in TOGETHER:
        spots = [(x, c) for x in xs for c in range(4)]
        spans = [pl.ds(max(4 * x + c - 1, 0), 2 if x + c else 1) for x, c in spots]
        states = attend(
            [q_block[4 * x + c] for x, c in spots],
            [k_block[span].reshape(-1, HEAD_DIM) for span in spans],
            [v_block[span].reshape(-1, HEAD_DIM) for span in spans],
            [bias[...] if x + c else bias[:, TILE:] for x, c in spots],
            [None] * len(spots),
        )
        for (x, c), state in zip(spots, states):
            for target, array in zip((top, total, acc), state):
                target[x, :, :, 8 * c : 8 * c + 8, :] = array.reshape(shape)

    set_bias(bias, order_two)
    shape = (4, STEPS, TILE)

    def rows(kind, x, res):
        return row[x, kind, :, res].reshape(TILE, HEAD_DIM)

    def span(kind, x, res):
        late = rows(kind, x, res)
        return jnp.concatenate([rows(kind, x - 1, res), late], axis=0) if x else late

    for xs in TOGETHER:
        spots = [(x, res) for x in xs for res in range(4)]
        states = attend(
            [rows(QUERY, x, res) for x, res in spots],
            [span(KEY, x, res) for x, res in spots],
            [span(VALUE, x, res) for x, res in spots],
            [bias[...] if x else bias[:, TILE:] for x, res in spots],
            [
                tuple(ref[x, :, res].reshape(TILE, TILE) for ref in (top, total, acc))
                for x, res in spots
            ],
        )
        for (x, res), state in zip(spots, states):
            for target, array in zip((top, total, acc), state):
                target[x, :, res] = array.reshape(shape)


def attend_own(row):
    state = jax.ShapeDtypeStruct((ROW_CHIPS, 4, 4, STEPS, HEAD_DIM), F32)
    return pl.pallas_call(
        own_kernel,
        out_shape=[state] * 3,
        in_specs=[VMEM],
        out_specs=[VMEM] * 3,
        scratch_shapes=[pltpu.VMEM((16, TILE, HEAD_DIM), BF16)] * 3
        + [pltpu.VMEM((TILE, 2 * TILE), F32)],
        compiler_params=room(16),
        cost_estimate=pl.CostEstimate(
            flops=1500000000, bytes_accessed=3000000, transcendentals=1000000
        ),
    )(row)


def back_kernel(
    place, row, back0, back1, back2, back3, top, total, acc, out,
    k_back, v_back, top0, total0, acc0, natural, bias,
):
    has_back = place[1] > 0
    for shift, back in enumerate((back0, back1, back2, back3)):
        source = (place[0] - shift) & 3
        k_back[source] = back[KEY]
        v_back[source] = back[VALUE]

    closed = jnp.where(has_back, 0.0, LOWEST).astype(F32)
    shape = (4, 4, 8, TILE)
    set_bias(bias, order_one)
    bias_one = bias[:, :TILE] + closed
    set_bias(bias, order_two)
    bias_two = bias[:, :TILE] + closed
    old = tuple(ref[0, :, :, 0:8, :].reshape(TILE, TILE) for ref in (top, total, acc))
    state, *states = attend(
        [split_blocks(row[0, QUERY])[0]]
        + [row[0, QUERY, :, res].reshape(TILE, HEAD_DIM) for res in range(4)],
        [split_blocks(k_back[3])[3]]
        + [k_back[3, :, res].reshape(TILE, HEAD_DIM) for res in range(4)],
        [split_blocks(v_back[3])[3]]
        + [v_back[3, :, res].reshape(TILE, HEAD_DIM) for res in range(4)],
        [bias_one] + [bias_two] * 4,
        [old] + [None] * 4,
    )
    for target, source, array in zip((top0, total0, acc0), (top, total, acc), state):
        target[:, :, 0:8, :] = array.reshape(shape)
        target[:, :, 8:, :] = source[0, :, :, 8:, :]
    olds = [
        tuple(ref[:, res].reshape(TILE, TILE) for ref in (top0, total0, acc0)) for res in range(4)
    ]
    for res, (new, old) in enumerate(zip(states, olds)):
        high = jnp.maximum(new[0], old[0])
        fade_new, fade_old = jnp.exp2(new[0] - high), jnp.exp2(old[0] - high)
        merged = [high] + [n * fade_new + o * fade_old for n, o in zip(new[1:], old[1:])]
        for target, array in zip((top0, total0, acc0), merged):
            target[:, res] = array.reshape(4, STEPS, TILE)

    set_bias(bias, order_three)
    bias[:, :TILE] = bias[:, :TILE] + closed

    def span(ref, kind, a, res):
        parts = (ref[:, a, res], row[:, kind, a, res])
        return jnp.concatenate([part.reshape(TILE, HEAD_DIM) for part in parts], axis=0)

    def state_of(near, far, a, res):
        rest = far[1:, a, res].reshape(3 * STEPS, TILE)
        return jnp.concatenate([near[a, res], rest], axis=0)

    for group in TOGETHER:
        spots = [(a, res) for a in group for res in range(4)]
        states = attend(
            [row[:, QUERY, a, res].reshape(TILE, HEAD_DIM) for a, res in spots],
            [span(k_back, KEY, a, res) for a, res in spots],
            [span(v_back, VALUE, a, res) for a, res in spots],
            [bias[...]] * len(spots),
            [
                tuple(
                    state_of(near, far, a, res)
                    for near, far in ((top0, top), (total0, total), (acc0, acc))
                )
                for a, res in spots
            ],
        )
        for (a, res), (_, count, part) in zip(spots, states):
            result = part / count
            for x in range(ROW_CHIPS):
                start = x * BLOCK + 4 * a + res
                natural[pl.ds(start, STEPS, stride=DILATION_THREE), :] = result[
                    x * STEPS : (x + 1) * STEPS
                ]
    out[...] = natural[...].astype(BF16)


def attend_back(place, row, backs, states):
    shape = (2, 4, 4, STEPS, HEAD_DIM)
    return pl.pallas_call(
        back_kernel,
        out_shape=jax.ShapeDtypeStruct((ROW_CHIPS * BLOCK, HEAD_DIM), BF16),
        in_specs=[SMEM] + [VMEM] * 8,
        out_specs=VMEM,
        scratch_shapes=[pltpu.VMEM((ROW_CHIPS, 4, 4, STEPS, HEAD_DIM), BF16)] * 2
        + [pltpu.VMEM((4, 4, STEPS, HEAD_DIM), F32)] * 3
        + [pltpu.VMEM((ROW_CHIPS * BLOCK, HEAD_DIM), F32), pltpu.VMEM((TILE, 2 * TILE), F32)],
        compiler_params=room(16),
        cost_estimate=pl.CostEstimate(
            flops=1000000000, bytes_accessed=3000000, transcendentals=600000
        ),
    )(place, row, *[back.reshape(shape) for back in backs], *states)


def first_half_kernel(place, mine, w, out):
    rows = pl.multiple_of(place[2] * BLOCK, BLOCK)
    features = jnp.concatenate([mine[head] for head in range(4)], axis=1)
    out[...] = jnp.dot(features, w[pl.ds(rows, BLOCK), :], preferred_element_type=F32)


def second_half_kernel(place, other, w, half, out, rounded, left):
    rows = pl.multiple_of((1 - place[2]) * BLOCK, BLOCK)
    part = w[pl.ds(rows, BLOCK), :]
    copies = []
    for tile in range(BLOCK // TILE):
        span = pl.ds(tile * TILE, TILE)
        features = jnp.concatenate([other[head, span] for head in range(4)], axis=1)
        rest = jnp.dot(features, part, preferred_element_type=F32)
        rounded[span, :] = (rest + half[span, :]).astype(BF16)
        copies.append(pltpu.make_async_copy(rounded.at[span], out.at[span], left.at[tile]))
        copies[-1].start()
    for copy in copies:
        copy.wait()


def project(place, features, w, half=None):
    columns = w.shape[1]
    last = half is not None
    operands = (features, w, half) if last else (features, w)
    scratch = [pltpu.VMEM((BLOCK, columns), BF16), pltpu.SemaphoreType.DMA((BLOCK // TILE,))]
    return pl.pallas_call(
        second_half_kernel if last else first_half_kernel,
        out_shape=jax.ShapeDtypeStruct((BLOCK, columns), BF16 if last else F32),
        in_specs=[SMEM] + [VMEM] * len(operands),
        out_specs=pl.BlockSpec(memory_space=pltpu.HBM) if last else VMEM,
        scratch_shapes=scratch if last else [],
        compiler_params=room(12),
        cost_estimate=pl.CostEstimate(
            flops=2 * BLOCK * BLOCK * columns, bytes_accessed=3000000, transcendentals=0
        ),
    )(place, *operands)


def local(queries, keys, values, w_out):
    rows = lax.axis_size("row")
    place = jnp.stack([lax.axis_index(name) for name in ("x", "row", "tp")]).astype(jnp.int32)

    def to_next_row(array, shift):
        route = [
            (row * ROW_CHIPS + x, (row + 1) * ROW_CHIPS + (x + shift) % ROW_CHIPS)
            for row in range(rows - 1)
            for x in range(ROW_CHIPS)
        ]
        return lax.ppermute(array, ("row", "x"), route)

    row_pack, *backs = pack(place, keys, values, queries)
    row = lax.all_to_all(row_pack, "x", 0, 0, tiled=True)
    backs = [to_next_row(back, shift) for shift, back in enumerate(backs)]
    row = row.reshape(ROW_CHIPS, 3, 4, 4, STEPS, HEAD_DIM)
    states = attend_own(row)
    attended = attend_back(place, row, backs, states)
    mine = lax.all_to_all(attended.reshape(ROW_CHIPS, BLOCK, HEAD_DIM), "x", 0, 0, tiled=True)
    other = lax.ppermute(mine, "tp", [(0, 1), (1, 0)])
    half = project(place, mine, w_out)
    return project(place, other, w_out, half)


def solution(mesh):
    rows = mesh.shape["sp"] // ROW_CHIPS
    grid = Mesh(mesh.devices.reshape(rows, ROW_CHIPS, mesh.shape["tp"]), ("row", "x", "tp"))
    whole = ("row", "x")
    in_specs = (P(whole, "tp", None),) * 3 + (P(None, "tp"),)
    return jax.shard_map(
        local, mesh=grid, in_specs=in_specs, out_specs=P(whole, "tp"), check_vma=False
    )
```
